32 devices in a mesh: rep: 2 (over x), fs: 4 (over z), tp: 4 (over y, core).
Axes of the slice: x: 2, y: 2, z: 4, core: 2. Of those that a mesh axis runs over, the one named last changes fastest.
Arguments:
- tokens: bfloat16 [8192, 2048], P(('rep', 'fs'), 'tp'), may hold values from -6 to 6
- mix_in_gain: bfloat16 [2048], replicated, may hold values from 0.099609375 to 1.8984375
- bgate_weight: bfloat16 [2048, 2048], P('fs', 'tp'), may hold values from -0.125 to 0.125
- cgate_weight: bfloat16 [2048, 2048], P('fs', 'tp'), may hold values from -0.125 to 0.125
- value_weight: bfloat16 [2048, 2048], P('fs', 'tp'), may hold values from -0.125 to 0.125
- conv_taps: bfloat16 [3, 2048], replicated, may hold values from -3 to 3
- out_weight: bfloat16 [2048, 2048], P('tp', 'fs'), may hold values from -0.41984465 to 0.41984465
- mix_out_gain: bfloat16 [2048], replicated, may hold values from 0.099609375 to 1.8984375
- ffn_in_gain: bfloat16 [2048], replicated, may hold values from 0.099609375 to 1.8984375
- up_weight: bfloat16 [2048, 8192], P('fs', 'tp'), may hold values from -0.125 to 0.125
- down_weight: bfloat16 [8192, 2048], P('tp', 'fs'), may hold values from -0.20992233 to 0.20992233
- ffn_out_gain: bfloat16 [2048], replicated, may hold values from 0.099609375 to 1.8984375
Outputs:
- result: bfloat16 [8192, 2048], P(('rep', 'fs'), 'tp')
The draws below stay inside these ranges and needn't reach their ends.
All inputs are finite; a program needn't handle non-finite values.
Results may differ from the reference program's by a relative error of at most 0.02.
Values may be sent and summed in bfloat16 or wider, within the bound.
A program may use at most 128 MiB of HBM per device.

```python
import jax
import jax.numpy as jnp
from jax import lax

D = 2048
CW = 2048
FF = 8192
LEN = 256
TOKENS = 8192
N_TP = 4


def rising_matrix(base, rows, cols, top):
    ramp = top ** (jnp.arange(cols, dtype=jnp.float32) / cols)
    return (base * ramp[None, :] * rows ** (-0.5)).astype(jnp.bfloat16)


def draw_out_weight(key, part):
    own_key = jax.random.fold_in(key, 11)
    base = jnp.clip(jax.random.normal(own_key, (CW, D), jnp.float32), -6.0, 6.0)
    return rising_matrix(base, CW, D, 3.0)


def draw_down_weight(key, part):
    own_key = jax.random.fold_in(key, 23)
    base = jnp.clip(jax.random.normal(own_key, (FF, D), jnp.float32), -6.0, 6.0)
    return rising_matrix(base, FF, D, 3.0)


def shard_levels(key, extent, split, least, top_value):
    def one(position, blocks):
        steps = jax.random.uniform(jax.random.fold_in(jax.random.fold_in(key, 6), position), (blocks,), jnp.float32, least / len(split), top_value / len(split))
        return jnp.repeat(jnp.exp(steps), extent[position] // blocks).reshape((-1,) + (1,) * (len(extent) - position - 1))

    level = one(*split[0])
    for cut in split[1:]:
        level = level * one(*cut)
    return level


def centred(key, extent, spread, reach, split=(), kind=jnp.bfloat16):
    level = shard_levels(key, extent, split, -0.22, 0.18) if split else 1.0
    drawn = jax.random.normal(key, extent, jnp.float32) * spread * level
    return jnp.minimum(jnp.maximum(drawn, -reach), reach).astype(kind)


def setup_inputs(seed: int = 0) -> dict:
    arg_keys = jax.random.split(jax.random.key(seed), 13)
    return {
        "tokens": centred(arg_keys[0], (TOKENS, D), 1.0, 6.0, ((0, 8), (1, 4))),
        "mix_in_gain": jnp.clip(1.0 + 0.18 * jax.random.normal(arg_keys[1], (D,), jnp.float32), 0.099609375, 1.8984375).astype(jnp.bfloat16),
        "bgate_weight": centred(arg_keys[2], (D, CW), D ** -0.5, 0.125, ((0, 4), (1, 4))),
        "cgate_weight": centred(arg_keys[3], (D, CW), D ** -0.5, 0.125, ((0, 4), (1, 4))),
        "value_weight": centred(arg_keys[4], (D, CW), D ** -0.5, 0.125, ((0, 4), (1, 4))),
        "conv_taps": centred(arg_keys[5], (3, CW), 0.6, 3.0),
        "out_weight": draw_out_weight(jax.random.fold_in(arg_keys[12], 71), 0),
        "mix_out_gain": jnp.clip(1.0 + 0.18 * jax.random.normal(arg_keys[7], (D,), jnp.float32), 0.099609375, 1.8984375).astype(jnp.bfloat16),
        "ffn_in_gain": jnp.clip(1.0 + 0.18 * jax.random.normal(arg_keys[8], (D,), jnp.float32), 0.099609375, 1.8984375).astype(jnp.bfloat16),
        "up_weight": centred(arg_keys[9], (D, FF), D ** -0.5, 0.125, ((0, 4), (1, 4))),
        "down_weight": draw_down_weight(jax.random.fold_in(arg_keys[12], 71), 0),
        "ffn_out_gain": jnp.clip(1.0 + 0.18 * jax.random.normal(arg_keys[11], (D,), jnp.float32), 0.099609375, 1.8984375).astype(jnp.bfloat16),
    }


epsilon = 1e-06

def normalize(rows, gain):
    rows = rows.astype(jnp.float32)
    factor = lax.rsqrt(lax.optimization_barrier(jnp.mean(rows * rows, axis=-1, keepdims=True)) + epsilon)
    return rows * factor * gain.astype(jnp.float32)

def block_sum(left, right, blocks):
    width = left.shape[1] // blocks

    def step(total, index):
        start = (index * width).astype(jnp.int32)
        piece_left = lax.dynamic_slice_in_dim(left, start, width, 1)
        piece_right = lax.dynamic_slice_in_dim(right, start, width, 0)
        partial_term = jnp.dot(piece_left, piece_right, preferred_element_type=jnp.float32).astype(jnp.bfloat16)
        return (total + partial_term.astype(jnp.float32), None)
    start_total = jnp.zeros((left.shape[0], right.shape[1]), jnp.float32)
    total, _ = lax.scan(step, start_total, jnp.arange(blocks, dtype=jnp.int32))
    return total

def convolve(inner, taps):
    seqs = inner.reshape(-1, LEN, inner.shape[1])
    padded = jnp.pad(seqs, ((0, 0), (1, 1), (0, 0)))
    weights = taps.astype(jnp.float32)
    out = weights[0] * padded[:, :-2] + weights[1] * padded[:, 1:-1] + weights[2] * padded[:, 2:]
    return out.reshape(inner.shape)

def reference(tokens, mix_in_gain, bgate_weight, cgate_weight, value_weight, conv_taps, out_weight, mix_out_gain, ffn_in_gain, up_weight, down_weight, ffn_out_gain):
    normed = normalize(tokens, mix_in_gain).astype(jnp.bfloat16)
    bgate = jnp.dot(normed, bgate_weight, preferred_element_type=jnp.float32).astype(jnp.bfloat16)
    cgate = jnp.dot(normed, cgate_weight, preferred_element_type=jnp.float32).astype(jnp.bfloat16)
    value = jnp.dot(normed, value_weight, preferred_element_type=jnp.float32).astype(jnp.bfloat16)
    inner = cgate.astype(jnp.float32) * value.astype(jnp.float32)
    gated = (bgate.astype(jnp.float32) * convolve(inner, conv_taps)).astype(jnp.bfloat16)
    mixed = block_sum(gated, out_weight, N_TP)
    resid = (tokens.astype(jnp.float32) + normalize(mixed, mix_out_gain)).astype(jnp.bfloat16)
    second = normalize(resid, ffn_in_gain).astype(jnp.bfloat16)
    lifted = jnp.dot(second, up_weight, preferred_element_type=jnp.float32)
    active = jnp.square(jnp.maximum(lifted, 0.0)).astype(jnp.bfloat16)
    ffn = block_sum(active, down_weight, N_TP)
    return (resid.astype(jnp.float32) + normalize(ffn, ffn_out_gain)).astype(jnp.bfloat16)
```

```python
import functools

import jax
import jax.numpy as jnp
from jax import lax
from jax.experimental import pallas as pl
from jax.experimental.pallas import tpu as pltpu
from jax.sharding import PartitionSpec as P

LEN = 256
LANES = 128
DOWN_BOTH = 2

epsilon = 1e-06
MESH = pl.DeviceIdType.MESH
F32 = jnp.float32
BF16 = jnp.bfloat16


def at(index, size):
    return pl.ds(pl.multiple_of(index * size, size), size)


def dot(left, right):
    return jnp.dot(left, right, preferred_element_type=F32)


def loop(low, high, fn):
    def one(i, carry):
        fn(i)
        return carry

    lax.fori_loop(low, high, one, 0)


def kernel(
    nfs, ntp, nu, nc, cw,
    tokens, gain1, wb, wc, wv, taps, wo, gain2, gain3, wu, wd, gain4,
    result,
    rows_w, out_w, down_w, big, active, land, pair, rs, acc, resid, fpart, fpair, frs, energy,
    recv_z, recv_x, send_r, send_l, send_x, local_sem, tok_local,
    ag_ys, ag_ds, ag_recv, land_send, land_recv,
    pair_send, pair_recv, rs_send, rs_recv, en_send, en_recv,
    fp_send, fp_recv, fr_send, fr_recv, back_send, back_recv,
):
    rep, fs, tp = lax.axis_index("rep"), lax.axis_index("fs"), lax.axis_index("tp")
    ny = ntp // 2
    core, y = lax.rem(tp, 2), tp // 2
    sibling = tp + 1 - 2 * core
    count, own = tokens.shape
    width = own * ntp
    seqs = count // LEN
    krows, chan = wb.shape
    hidden = wu.shape[1]
    ucol = hidden // nu
    ocol = wo.shape[1]
    block = nfs * cw
    piece = block // ntp
    odd = lax.rem(fs, 2)
    worker = jnp.where(fs < nfs // 2, odd, 1 - odd) == 1
    partner = fs + 1 - 2 * odd
    end = (fs == 0) | (fs == nfs - 1)

    barrier = pltpu.get_barrier_semaphore()
    for step in (1, nfs - 1):
        pl.semaphore_signal(barrier, inc=1, device_id={"fs": lax.rem(fs + step, nfs)}, device_id_type=MESH)
    pl.semaphore_signal(barrier, inc=1, device_id={"rep": 1 - rep}, device_id_type=MESH)
    for step in range(1, ntp):
        pl.semaphore_signal(barrier, inc=1, device_id={"tp": lax.rem(tp + step, ntp)}, device_id_type=MESH)
    pl.semaphore_wait(barrier, 3 + ntp - 1)

    def slot(kind, j):
        return {"mix": j, "out": 3, "up": 4 + j, "down": 4 + nu + j}[kind]

    def ends(kind):
        return (0, nfs - 1) if kind in ("mix", "out") else (1, nfs - 2)

    def region(kind, j, s, half):
        if kind in ("mix", "up"):
            index = j if kind == "mix" else 3 + j
            if half is None:
                return rows_w.at[index, at(s, krows), :]
            return rows_w.at[index, at(s * 2 + half, krows // 2), :]
        if kind == "out":
            r = slice(None) if half is None else at(half, wo.shape[0] // 2)
            return out_w.at[r, at(s, ocol)]
        r = slice(None) if half is None else at(half, wd.shape[0] // 2)
        return down_w.at[j, r, at(s, cw)]

    def source(kind, j, half):
        if kind == "mix":
            ref, c = (wb, wc, wv)[j], slice(None)
        elif kind == "out":
            ref, c = wo, slice(None)
        elif kind == "up":
            ref, c = wu, at(j, ucol)
        else:
            ref, c = wd, at(j, cw)
        r = slice(None) if half is None else at(half, ref.shape[0] // 2)
        return ref.at[r, c]

    def hop(kind, j, s, mine, sems, to):
        k = slot(kind, j)
        src = source(kind, j, rep) if mine else region(kind, j, s, rep)
        return pltpu.make_async_remote_copy(
            src, region(kind, j, s, rep), sems.at[k, s], recv_z.at[k, s],
            device_id={"fs": to}, device_id_type=MESH)

    def right(kind, j, s, mine=False):
        return hop(kind, j, s, mine, send_r, lax.rem(fs + 1, nfs))

    def left(kind, j, s, mine=False):
        return hop(kind, j, s, mine, send_l, lax.rem(fs + nfs - 1, nfs))

    def across(kind, j, s, half):
        k = slot(kind, j)
        return pltpu.make_async_remote_copy(
            region(kind, j, s, half), region(kind, j, s, half), send_x.at[k, s], recv_x.at[k, s],
            device_id={"rep": 1 - rep}, device_id_type=MESH)

    def extra(kind, j):
        k = slot(kind, j)
        to = jnp.where(fs == 0, 1, nfs - 2)
        return pltpu.make_async_remote_copy(
            source(kind, j, 1 - rep), region(kind, j, fs, 1 - rep), send_x.at[k, fs], recv_x.at[k, fs],
            device_id={"fs": to}, device_id_type=MESH)

    def both(kind, j):
        return j < DOWN_BOTH if kind == "down" else True

    def crosses(kind, j, s):
        near = ((s == 0) & (fs == 1)) | ((s == nfs - 1) & (fs == nfs - 2))
        keep = jnp.logical_not(near & both(kind, j)) & (s != fs)
        return keep if kind in ("mix", "out") else keep & worker

    def send_own(kind, j):
        low, high = ends(kind)

        @pl.when(fs < high)
        def _():
            right(kind, j, fs, True).start()

        @pl.when(fs > low)
        def _():
            left(kind, j, fs, True).start()

        @pl.when(end & both(kind, j))
        def _():
            extra(kind, j).start()

    def local(kind, j):
        return pltpu.make_async_copy(source(kind, j, None), region(kind, j, fs, None), local_sem.at[slot(kind, j)])

    def relay(kind, j):
        low, high = ends(kind)
        inside = (fs >= low) & (fs <= high)

        def one(d):
            @pl.when((fs - d >= 0) & inside)
            def _():
                s = fs - d
                right(kind, j, s).wait_recv()

                @pl.when(fs < high)
                def _():
                    right(kind, j, s).start()

                @pl.when(crosses(kind, j, s))
                def _():
                    across(kind, j, s, rep).start()

            @pl.when((fs + d < nfs) & inside)
            def _():
                s = fs + d
                left(kind, j, s).wait_recv()

                @pl.when(fs > low)
                def _():
                    left(kind, j, s).start()

                @pl.when(crosses(kind, j, s))
                def _():
                    across(kind, j, s, rep).start()

        loop(1, nfs, one)

    def complete(kind, j):
        def one(s):
            @pl.when(s != fs)
            def _():
                across(kind, j, s, 1 - rep).wait_recv()

        loop(0, nfs, one)
        local(kind, j).wait()

    def drain(kind, j):
        low, high = ends(kind)

        def one(s):
            @pl.when((s <= fs) & (fs < high))
            def _():
                right(kind, j, s).wait_send()

            @pl.when((s >= fs) & (fs > low))
            def _():
                left(kind, j, s).wait_send()

            inside = (fs >= low) & (fs <= high)

            @pl.when(crosses(kind, j, s) & inside)
            def _():
                across(kind, j, s, rep).wait_send()

        loop(0, nfs, one)

        @pl.when(end & both(kind, j))
        def _():
            extra(kind, j).wait_send()

    def group(to, src, dst, send, recv):
        return pltpu.make_async_remote_copy(
            src, dst, send, recv, device_id={"tp": to}, device_id_type=MESH)

    def up_y(t):
        return lax.rem(y + t, ny) * 2 + core

    def down_y(t):
        return lax.rem(y + ny - t, ny) * 2 + core

    def gathered(j, i, who):
        return big.at[min(j, 1), at(i, LEN), at(who, own)]

    def ag_y(j, i, t):
        src = tokens.at[at(i, LEN), :] if j == 2 else gathered(j, i, tp)
        return group(up_y(t), src, gathered(j, i, tp), ag_ys.at[j, i, t - 1], ag_recv.at[j, i, tp])

    def ag_pair(j, i):
        src = tokens.at[at(i, LEN), :] if j == 2 else gathered(j, i, tp)
        return group(sibling, src, gathered(j, i, tp), ag_ds.at[j, i, 0], ag_recv.at[j, i, tp])

    def ag_relay(j, i, t):
        who = down_y(t)
        return group(sibling, gathered(j, i, who), gathered(j, i, who), ag_ds.at[j, i, t], ag_recv.at[j, i, who])

    def ag_start(j, i):
        for t in range(1, ny):
            ag_y(j, i, t).start()
        ag_pair(j, i).start()

    def ag_pass(j, i):
        for t in range(1, ny):
            ag_relay(j, i, t).wait_recv()
            ag_relay(j, i, t).start()

    def ag_finish(j, i):
        for t in range(ny):
            who = lax.rem(y + t, ny) * 2 + 1 - core
            group(sibling, gathered(j, i, who), gathered(j, i, who), ag_ds.at[j, i, 0], ag_recv.at[j, i, who]).wait_recv()

    def ag_drain(j, i):
        for t in range(1, ny):
            ag_y(j, i, t).wait_send()
            ag_relay(j, i, t).wait_send()
        ag_pair(j, i).wait_send()

    def hand(i):
        return pltpu.make_async_remote_copy(
            land.at[at(i, LEN), :], land.at[at(i, LEN), :], land_send.at[i], land_recv.at[i],
            device_id={"fs": partner}, device_id_type=MESH)

    def pair_copy(i, b):
        src = active.at[1, at(i, LEN), at(2 * b + 1 - core, own)]
        return group(sibling, src, pair.at[b, at(i, LEN), :], pair_send.at[i, b], pair_recv.at[i, b])

    def rs_copy(i, t):
        src = pair.at[lax.rem(y + t, ny), at(i, LEN), :]
        return group(up_y(t), src, rs.at[t - 1, at(i, LEN), :], rs_send.at[i, t - 1], rs_recv.at[i, t - 1])

    def en_copy(stage, i, t):
        return group(
            lax.rem(tp + t, ntp), energy.at[stage, 0, i], energy.at[stage, t, i],
            en_send.at[stage, i, t - 1], en_recv.at[stage, i, t - 1])

    def en_put(stage, i, values):
        square = jnp.sum(values * values, axis=1, keepdims=True)
        flat = jnp.transpose(jnp.broadcast_to(square, (LEN, LANES)))
        energy[stage, 0, i] = flat[0:8, :]
        for t in range(1, ntp):
            en_copy(stage, i, t).start()

    def en_get(stage, i):
        for t in range(1, ntp):
            en_copy(stage, i, t).wait_recv()
        flat = energy[stage, 0, i]
        for t in range(1, ntp):
            flat = flat + energy[stage, t, i]
        tall = jnp.transpose(jnp.concatenate([flat] * (LANES // 8), axis=0))
        return lax.rsqrt(tall[:, 0:1] / width + epsilon)

    def fp_copy(c, j, i):
        return group(
            sibling, fpart.at[lax.rem(c, 2), j, :, 1 - core, at(i, LEN), :], fpair.at[j, c, :, at(i, LEN), :],
            fp_send.at[j, c, i], fp_recv.at[j, c, i])

    def fr_copy(c, i, t):
        src = fpair.at[0, c, lax.rem(y + t, ny), at(i, LEN), :]
        return group(up_y(t), src, frs.at[t - 1, c, at(i, LEN), :], fr_send.at[c, i, t - 1], fr_recv.at[c, i, t - 1])

    def back(c, i):
        return pltpu.make_async_remote_copy(
            fpair.at[1, c, :, at(i, LEN), :], fpair.at[0, c, :, at(i, LEN), :], back_send.at[c, i], back_recv.at[c, i],
            device_id={"fs": partner}, device_id_type=MESH)

    send_own("mix", 0)
    loop(0, seqs, lambda i: ag_start(2, i))
    own_tok = pltpu.make_async_copy(tokens, big.at[1, :, at(tp, own)], tok_local)
    own_tok.start()
    send_own("mix", 1)
    for k in range(3):
        local("mix", k).start()
    local("out", 0).start()

    @pl.when(worker)
    def _():
        loop(0, nu, lambda j: local("up", j).start())
        loop(0, nc, lambda j: local("down", j).start())

    relay("mix", 0)
    send_own("mix", 2)
    loop(0, seqs, lambda i: ag_pass(2, i))
    relay("mix", 1)
    send_own("out", 0)
    own_tok.wait()

    def norm_tokens(i):
        ag_finish(2, i)
        r = at(i, LEN)
        v = big[1, r, :].astype(F32)
        factor = lax.rsqrt(jnp.mean(v * v, axis=-1, keepdims=True) + epsilon)
        big[0, r, :] = (v * factor * gain1[...].astype(F32)).astype(BF16)

    loop(0, seqs, norm_tokens)
    relay("mix", 2)
    send_own("up", 0)
    for k in range(3):
        complete("mix", k)

    own_taps = taps[:, at(tp, chan)].astype(F32)
    position = lax.broadcasted_iota(jnp.int32, (LEN, chan), 0)

    def mixer(i):
        r = at(i, LEN)
        rows = big[0, r, :]
        inner = dot(rows, rows_w[1]).astype(BF16).astype(F32) * dot(rows, rows_w[2]).astype(BF16).astype(F32)
        before = jnp.where(position == 0, 0.0, pltpu.roll(inner, 1, 0))
        after = jnp.where(position == LEN - 1, 0.0, pltpu.roll(inner, LEN - 1, 0))
        conv = own_taps[0:1] * before + own_taps[1:2] * inner + own_taps[2:3] * after
        outer = dot(rows, rows_w[0]).astype(BF16).astype(F32)
        active[0, r, 0:chan] = (outer * conv).astype(BF16)

        @pl.when(i == seqs // 2)
        def _():
            relay("out", 0)
            send_own("up", min(1, nu - 1)) if nu > 1 else None

    loop(0, seqs, mixer)
    complete("out", 0)

    def project(i):
        r = at(i, LEN)

        @pl.when(i < seqs)
        def _():
            active[1, r, 0:width] = dot(active[0, r, 0:chan], out_w[...]).astype(BF16)
            for b in range(ny):
                pair_copy(i, b).start()

        @pl.when(i > 0)
        def _():
            last = i - 1
            r = at(last, LEN)
            for b in range(ny):
                pair_copy(last, b).wait_recv()
                total = active[1, r, at(2 * b + core, own)].astype(F32) + pair[b, r, :].astype(F32)
                pair[b, r, :] = total.astype(BF16)
            for t in range(1, ny):
                rs_copy(last, t).start()

    loop(0, seqs + 1, project)
    loop(0, seqs, lambda i: ag_drain(2, i))

    own_gain2 = gain2[:, at(tp, own)].astype(F32)
    own_gain3 = gain3[:, at(tp, own)].astype(F32)

    def mixed_sum(i):
        r = at(i, LEN)
        total = pair[y, r, :].astype(F32)
        for t in range(1, ny):
            rs_copy(i, t).wait_recv()
            total = total + rs[t - 1, r, :].astype(F32)
        acc[r, :] = total
        en_put(0, i, total)

    def add_resid(i):
        r = at(i, LEN)
        scale = en_get(0, i)
        res = (big[1, r, at(tp, own)].astype(F32) + acc[r, :] * scale * own_gain2).astype(BF16)
        resid[r, :] = res
        en_put(1, i, res.astype(F32))

    def normalise(i):
        r = at(i, LEN)
        rows = (resid[r, :].astype(F32) * en_get(1, i) * own_gain3).astype(BF16)

        @pl.when(worker)
        def _():
            big[0, r, at(tp, own)] = rows
            ag_start(0, i)

        @pl.when(jnp.logical_not(worker))
        def _():
            land[r, :] = rows
            hand(i).start()

    first = min(2, nu)

    def exchange(step):
        @pl.when(step < nu)
        def _():
            @pl.when(step + first < nu)
            def _():
                send_own("up", step + first)

            @pl.when(step == nu - 1)
            def _():
                send_own("down", 0)

            relay("up", step)

        @pl.when(step < seqs)
        def _():
            mixed_sum(step)

        @pl.when((step >= 1) & (step < seqs + 1))
        def _():
            add_resid(step - 1)

        @pl.when((step >= 2) & (step < seqs + 2))
        def _():
            normalise(step - 2)

        @pl.when((step >= 3) & (step < seqs + 3) & worker)
        def _():
            ag_pass(0, step - 3)

    loop(0, max(seqs + 3, nu), exchange)
    for i in range(seqs):
        for b in range(ny):
            pair_copy(i, b).wait_send()

    def sum_pair(c, j, i):
        r = at(i, LEN)
        fp_copy(c, j, i).wait_recv()
        for b in range(ny):
            total = fpart[lax.rem(c, 2), j, b, core, r, :].astype(F32) + fpair[j, c, b, r, :].astype(F32)
            fpair[j, c, b, r, :] = total.astype(BF16)

    def fr_start(c, i):
        for t in range(1, ny):
            fr_copy(c, i, t).start()

    @pl.when(jnp.logical_not(worker))
    def _():
        loop(1, nc, lambda c: send_own("down", c))

        def returned(c):
            def one(i):
                back(c, i).wait_recv()
                fr_start(c, i)

            loop(0, seqs, one)

        loop(0, nc, returned)

    @pl.when(worker)
    def _():
        loop(0, nu, lambda j: complete("up", j))

        def lift(j, i):
            ag_finish(j, i)
            r = at(i, LEN)
            rows = big[j, r, :]
            for u in range(nu):
                lifted = jnp.maximum(dot(rows, rows_w[3 + u]), 0.0)
                active[j, r, pl.ds(u * ucol, ucol)] = (lifted * lifted).astype(BF16)

        early = min(nc, seqs // 2)

        def pump(c):
            @pl.when(c + 1 < nc)
            def _():
                send_own("down", c + 1)

            relay("down", c)

        def own_rows(i):
            lift(0, i)
            hand(i).wait_recv()
            r = at(i, LEN)
            big[1, r, at(tp, own)] = land[r, :]
            ag_start(1, i)

            @pl.when(i > 0)
            def _():
                ag_pass(1, i - 1)

            @pl.when((lax.rem(i, 2) == 1) & (i // 2 < early))
            def _():
                pump(i // 2)

        loop(0, seqs, own_rows)
        ag_pass(1, seqs - 1)

        def partner_rows(i):
            lift(1, i)
            if early < nc:
                @pl.when(i == seqs // 2)
                def _():
                    pump(early)

        loop(0, seqs, partner_rows)
        ready = min(early + 1, nc)
        lag = 2

        def chunk(c):
            @pl.when((c + 1 >= ready) & (c + 1 < nc))
            def _():
                pump(c + 1)

            complete("down", c)

            def unit(n):
                @pl.when(n < 2 * seqs)
                def _():
                    j, i = 1 - n // seqs, lax.rem(n, seqs)
                    r = at(i, LEN)

                    @pl.when(c >= 2)
                    def _():
                        fp_copy(c - 2, j, i).wait_send()

                    product = dot(active[j, r, 0:hidden], down_w[c]).astype(BF16)
                    for b in range(ny):
                        for half in range(2):
                            lane = (2 * b + half) * piece
                            fpart[lax.rem(c, 2), j, b, half, r, :] = product[:, lane:lane + piece]
                    fp_copy(c, j, i).start()

                @pl.when(n >= lag)
                def _():
                    m = n - lag
                    j, i = 1 - m // seqs, lax.rem(m, seqs)
                    sum_pair(c, j, i)

                    @pl.when(j == 0)
                    def _():
                        fr_start(c, i)

                    @pl.when(j == 1)
                    def _():
                        back(c, i).start()

            loop(0, 2 * seqs + lag, unit)

        loop(0, nc, chunk)

    own_gain4 = gain4[:, at(tp, own)].astype(F32)

    def close(step):
        @pl.when(step < seqs)
        def _():
            r = at(step, LEN)
            parts = []
            for c in range(nc):
                total = fpair[0, c, y, r, :].astype(F32)
                for t in range(1, ny):
                    fr_copy(c, step, t).wait_recv()
                    total = total + frs[t - 1, c, r, :].astype(F32)
                parts.append(total)
            total = parts[0] if nc == 1 else jnp.concatenate(parts, axis=1)
            acc[r, :] = total
            en_put(2, step, total)

        @pl.when(step > 0)
        def _():
            r = at(step - 1, LEN)
            scale = en_get(2, step - 1)
            result[r, :] = (resid[r, :].astype(F32) + acc[r, :] * scale * own_gain4).astype(BF16)

    loop(0, seqs + 1, close)

    for k in range(3):
        drain("mix", k)
    drain("out", 0)
    loop(0, nu, lambda j: drain("up", j))
    loop(0, nc, lambda j: drain("down", j))

    def finish(i):
        for t in range(1, ny):
            rs_copy(i, t).wait_send()
            loop(0, nc, lambda c: fr_copy(c, i, t).wait_send())
        for stage in range(3):
            for t in range(1, ntp):
                en_copy(stage, i, t).wait_send()

        @pl.when(worker)
        def _():
            ag_drain(0, i)
            ag_drain(1, i)
            for j in range(2):
                loop(max(nc - 2, 0), nc, lambda c: fp_copy(c, j, i).wait_send())
            loop(0, nc, lambda c: back(c, i).wait_send())

        @pl.when(jnp.logical_not(worker))
        def _():
            hand(i).wait_send()

    loop(0, seqs, finish)


def solution(mesh):
    nfs, ntp = mesh.shape["fs"], mesh.shape["tp"]
    assert mesh.shape["rep"] == 2 and nfs % 2 == 0 and nfs >= 4 and ntp % 2 == 0

    def body(tokens, gain1, wb, wc, wv, taps, wo, gain2, gain3, wu, wd, gain4):
        count, own = tokens.shape
        width, chan, hidden = own * ntp, wb.shape[1], wu.shape[1]
        nu = hidden // chan
        cw = min(LANES, wd.shape[1])
        nc = wd.shape[1] // cw
        nk = 4 + nu + nc
        ny, seqs = ntp // 2, count // LEN
        piece = nfs * cw // ntp
        vm, anyw = pl.BlockSpec(memory_space=pltpu.VMEM), pl.BlockSpec(memory_space=pl.ANY)
        dma = pltpu.SemaphoreType.DMA
        return pl.pallas_call(
            functools.partial(kernel, nfs, ntp, nu, nc, cw),
            out_shape=jax.ShapeDtypeStruct((count, own), BF16),
            in_specs=[anyw, vm, anyw, anyw, anyw, vm, anyw, vm, vm, anyw, anyw, vm],
            out_specs=vm,
            scratch_shapes=[
                pltpu.VMEM((3 + nu, width, chan), BF16),
                pltpu.VMEM((chan, width), BF16),
                pltpu.VMEM((nc, hidden, nfs * cw), BF16),
                pltpu.VMEM((2, count, width), BF16),
                pltpu.VMEM((2, count, max(hidden, width)), BF16),
                pltpu.VMEM((count, own), BF16),
                pltpu.VMEM((ny, count, own), BF16),
                pltpu.VMEM((ny - 1, count, own), BF16),
                pltpu.VMEM((count, own), F32),
                pltpu.VMEM((count, own), BF16),
                pltpu.VMEM((2, 2, ny, 2, count, piece), BF16),
                pltpu.VMEM((2, nc, ny, count, piece), BF16),
                pltpu.VMEM((ny - 1, nc, count, piece), BF16),
                pltpu.VMEM((3, ntp, seqs, 8, LEN), F32),
                dma((nk, nfs)), dma((nk, nfs)), dma((nk, nfs)), dma((nk, nfs)), dma((nk, nfs)),
                dma((nk,)), dma,
                dma((3, seqs, ny - 1)), dma((3, seqs, ny)), dma((3, seqs, ntp)), dma((seqs,)), dma((seqs,)),
                dma((seqs, ny)), dma((seqs, ny)), dma((seqs, ny - 1)), dma((seqs, ny - 1)),
                dma((3, seqs, ntp - 1)), dma((3, seqs, ntp - 1)),
                dma((2, nc, seqs)), dma((2, nc, seqs)), dma((nc, seqs, ny - 1)), dma((nc, seqs, ny - 1)),
                dma((nc, seqs)), dma((nc, seqs)),
            ],
            compiler_params=pltpu.CompilerParams(
                collective_id=0, has_side_effects=True, vmem_limit_bytes=66000000),
            name="layer",
        )(tokens, gain1[None], wb, wc, wv, taps, wo, gain2[None], gain3[None], wu, wd, gain4[None])

    placed = (
        P(("rep", "fs"), "tp"), P(), P("fs", "tp"), P("fs", "tp"), P("fs", "tp"), P(), P("tp", "fs"),
        P(), P(), P("fs", "tp"), P("tp", "fs"), P(),
    )
    return jax.shard_map(
        body, mesh=mesh, in_specs=placed, out_specs=P(("rep", "fs"), "tp"), check_vma=False
    )
```

```python
import functools

import jax
import jax.numpy as jnp
from jax import lax
from jax.experimental import pallas as pl
from jax.experimental.pallas import tpu as pltpu
from jax.sharding import PartitionSpec as P

LEN = 256
LANES = 128
DOWN_BOTH = 2

epsilon = 1e-06
MESH = pl.DeviceIdType.MESH
F32 = jnp.float32
BF16 = jnp.bfloat16


def at(index, size):
    return pl.ds(pl.multiple_of(index * size, size), size)


def dot(left, right):
    return jnp.dot(left, right, preferred_element_type=F32)


def row(v):
    return v.astype(F32).reshape(1, v.shape[0])


def early_chunks(nc):
    return min(2, nc - 1)


def loop(low, high, fn):
    def one(i, carry):
        fn(i)
        return carry

    lax.fori_loop(low, high, one, 0)


def kernel(
    nfs, ntp, nu, nc, cw,
    tokens, gain1, wb, wc, wv, taps, wo, gain2, gain3, wu, wd, gain4,
    result,
    rows_w, out_w, down_w, big, active, land, pair, rs, acc, resid, fpart, fpair, frs, fsum, energy,
    recv_z, recv_x, send_r, send_l, send_x, local_sem, tok_local,
    ag_ys, ag_ds, ag_recv, land_send, land_recv,
    pair_send, pair_recv, rs_send, rs_recv, en_send, en_recv,
    fp_send, fp_recv, fr_send, fr_recv, back_send, back_recv, fs_send, fs_recv,
):
    rep, fs, tp = lax.axis_index("rep"), lax.axis_index("fs"), lax.axis_index("tp")
    ny = ntp // 2
    core, y = lax.rem(tp, 2), tp // 2
    sibling = tp + 1 - 2 * core
    count, own = tokens.shape
    width = own * ntp
    seqs = count // LEN
    krows, chan = wb.shape
    hidden = wu.shape[1]
    ucol = hidden // nu
    ocol = wo.shape[1]
    nk = 4 + nu + nc
    n_early = early_chunks(nc)
    block = nfs * cw
    piece = block // ntp
    odd = lax.rem(fs, 2)
    worker = jnp.where(fs < nfs // 2, odd, 1 - odd) == 1
    partner = fs + 1 - 2 * odd
    end = (fs == 0) | (fs == nfs - 1)

    barrier = pltpu.get_barrier_semaphore()
    for step in (1, nfs - 1):
        pl.semaphore_signal(barrier, inc=1, device_id={"fs": lax.rem(fs + step, nfs)}, device_id_type=MESH)
    pl.semaphore_signal(barrier, inc=1, device_id={"rep": 1 - rep}, device_id_type=MESH)
    for step in range(1, ntp):
        pl.semaphore_signal(barrier, inc=1, device_id={"tp": lax.rem(tp + step, ntp)}, device_id_type=MESH)
    pl.semaphore_wait(barrier, 3 + ntp - 1)

    def slot(kind, j):
        return {"mix": j, "out": 3, "up": 4 + j, "down": 4 + nu + j}[kind]

    def ends(kind):
        return (0, nfs - 1) if kind in ("mix", "out") else (1, nfs - 2)

    def region(kind, j, s, half):
        if kind in ("mix", "up"):
            index = j if kind == "mix" else 3 + j
            if half is None:
                return rows_w.at[index, at(s, krows), :]
            return rows_w.at[index, at(s * 2 + half, krows // 2), :]
        if kind == "out":
            r = slice(None) if half is None else at(half, wo.shape[0] // 2)
            return out_w.at[r, at(s, ocol)]
        r = slice(None) if half is None else at(half, wd.shape[0] // 2)
        return down_w.at[j, r, at(s, cw)]

    def source(kind, j, half):
        if kind == "mix":
            ref, c = (wb, wc, wv)[j], slice(None)
        elif kind == "out":
            ref, c = wo, slice(None)
        elif kind == "up":
            ref, c = wu, at(j, ucol)
        else:
            ref, c = wd, at(j, cw)
        r = slice(None) if half is None else at(half, ref.shape[0] // 2)
        return ref.at[r, c]

    def hop(kind, j, s, mine, sems, to):
        k = slot(kind, j)
        src = source(kind, j, rep) if mine else region(kind, j, s, rep)
        return pltpu.make_async_remote_copy(
            src, region(kind, j, s, rep), sems.at[k, s], recv_z.at[k, s],
            device_id={"fs": to}, device_id_type=MESH)

    def right(kind, j, s, mine=False):
        return hop(kind, j, s, mine, send_r, lax.rem(fs + 1, nfs))

    def left(kind, j, s, mine=False):
        return hop(kind, j, s, mine, send_l, lax.rem(fs + nfs - 1, nfs))

    def across(kind, j, s, half):
        k = slot(kind, j)
        return pltpu.make_async_remote_copy(
            region(kind, j, s, half), region(kind, j, s, half), send_x.at[k, s], recv_x.at[k, s],
            device_id={"rep": 1 - rep}, device_id_type=MESH)

    def extra(kind, j, src):
        k = slot(kind, j)
        to = jnp.where(fs == 0, 1, nfs - 2)
        return pltpu.make_async_remote_copy(
            src, region(kind, j, fs, 1 - rep), send_x.at[k, fs], recv_x.at[k, fs],
            device_id={"fs": to}, device_id_type=MESH)

    def both(kind, j):
        return j < DOWN_BOTH if kind == "down" else True

    def crosses(kind, j, s):
        near = ((s == 0) & (fs == 1)) | ((s == nfs - 1) & (fs == nfs - 2))
        keep = jnp.logical_not(near & both(kind, j)) & (s != fs)
        return keep if kind in ("mix", "out") else keep & worker

    def send_own(kind, j):
        low, high = ends(kind)

        @pl.when(fs < high)
        def _():
            right(kind, j, fs, True).start()

        @pl.when(fs > low)
        def _():
            left(kind, j, fs, True).start()

        @pl.when(end & both(kind, j))
        def _():
            extra(kind, j, source(kind, j, 1 - rep)).start()

    def local(kind, j):
        return pltpu.make_async_copy(source(kind, j, None), region(kind, j, fs, None), local_sem.at[slot(kind, j)])

    def relay(kind, j, first, last, mid=True, out=True):
        low, high = ends(kind)
        inside = (fs >= low) & (fs <= high)
        lower = fs < nfs // 2
        from_left = inside & ((lower & out) | (jnp.logical_not(lower) & mid))
        from_right = inside & ((lower & mid) | (jnp.logical_not(lower) & out))

        def one(d):
            @pl.when((fs - d >= 0) & from_left)
            def _():
                s = fs - d
                right(kind, j, s).wait_recv()

                @pl.when(fs < high)
                def _():
                    right(kind, j, s).start()

                @pl.when(crosses(kind, j, s))
                def _():
                    across(kind, j, s, rep).start()

            @pl.when((fs + d < nfs) & from_right)
            def _():
                s = fs + d
                left(kind, j, s).wait_recv()

                @pl.when(fs > low)
                def _():
                    left(kind, j, s).start()

                @pl.when(crosses(kind, j, s))
                def _():
                    across(kind, j, s, rep).start()

        loop(first, last, one)

    def complete(kind, j):
        def one(s):
            @pl.when(s != fs)
            def _():
                across(kind, j, s, 1 - rep).wait_recv()

        loop(0, nfs, one)
        local(kind, j).wait()

    def drain(kind, j):
        low, high = ends(kind)

        def one(s):
            @pl.when((s <= fs) & (fs < high))
            def _():
                right(kind, j, s).wait_send()

            @pl.when((s >= fs) & (fs > low))
            def _():
                left(kind, j, s).wait_send()

            inside = (fs >= low) & (fs <= high)

            @pl.when(crosses(kind, j, s) & inside)
            def _():
                across(kind, j, s, rep).wait_send()

        loop(0, nfs, one)

        @pl.when(end & both(kind, j))
        def _():
            extra(kind, j, region(kind, j, fs, 1 - rep)).wait_send()

    def group(to, src, dst, send, recv):
        return pltpu.make_async_remote_copy(
            src, dst, send, recv, device_id={"tp": to}, device_id_type=MESH)

    def up_y(t):
        return lax.rem(y + t, ny) * 2 + core

    def down_y(t):
        return lax.rem(y + ny - t, ny) * 2 + core

    def gathered(j, i, who):
        return big.at[min(j, 1), at(i, LEN), at(who, own)]

    def ag_y(j, i, t):
        src = tokens.at[at(i, LEN), :] if j == 2 else gathered(j, i, tp)
        return group(up_y(t), src, gathered(j, i, tp), ag_ys.at[j, i, t - 1], ag_recv.at[j, i, tp])

    def ag_pair(j, i):
        src = tokens.at[at(i, LEN), :] if j == 2 else gathered(j, i, tp)
        return group(sibling, src, gathered(j, i, tp), ag_ds.at[j, i, 0], ag_recv.at[j, i, tp])

    def ag_relay(j, i, t):
        who = down_y(t)
        return group(sibling, gathered(j, i, who), gathered(j, i, who), ag_ds.at[j, i, t], ag_recv.at[j, i, who])

    def ag_start(j, i):
        for t in range(1, ny):
            ag_y(j, i, t).start()
        ag_pair(j, i).start()

    def ag_pass(j, i):
        for t in range(1, ny):
            ag_relay(j, i, t).wait_recv()
            ag_relay(j, i, t).start()

    def ag_finish(j, i):
        for t in range(ny):
            who = lax.rem(y + t, ny) * 2 + 1 - core
            group(sibling, gathered(j, i, who), gathered(j, i, who), ag_ds.at[j, i, 0], ag_recv.at[j, i, who]).wait_recv()

    def ag_drain(j, i):
        for t in range(1, ny):
            ag_y(j, i, t).wait_send()
            ag_relay(j, i, t).wait_send()
        ag_pair(j, i).wait_send()

    def hand(i):
        return pltpu.make_async_remote_copy(
            land.at[at(i, LEN), :], land.at[at(i, LEN), :], land_send.at[i], land_recv.at[i],
            device_id={"fs": partner}, device_id_type=MESH)

    def pair_copy(i, b):
        src = active.at[1, at(i, LEN), at(2 * b + 1 - core, own)]
        return group(sibling, src, pair.at[b, at(i, LEN), :], pair_send.at[i, b], pair_recv.at[i, b])

    def rs_copy(i, t):
        src = pair.at[lax.rem(y + t, ny), at(i, LEN), :]
        return group(up_y(t), src, rs.at[t - 1, at(i, LEN), :], rs_send.at[i, t - 1], rs_recv.at[i, t - 1])

    def en_copy(stage, i, t):
        return group(
            lax.rem(tp + t, ntp), energy.at[stage, 0, i], energy.at[stage, t, i],
            en_send.at[stage, i, t - 1], en_recv.at[stage, i, t - 1])

    def en_put(stage, i, values):
        square = jnp.sum(values * values, axis=1, keepdims=True)
        flat = jnp.transpose(jnp.broadcast_to(square, (LEN, LANES)))
        energy[stage, 0, i] = flat[0:8, :]
        for t in range(1, ntp):
            en_copy(stage, i, t).start()

    def en_get(stage, i):
        for t in range(1, ntp):
            en_copy(stage, i, t).wait_recv()
        flat = energy[stage, 0, i]
        for t in range(1, ntp):
            flat = flat + energy[stage, t, i]
        tall = jnp.transpose(jnp.concatenate([flat] * (LANES // 8), axis=0))
        return lax.rsqrt(tall[:, 0:1] / width + epsilon)

    def fp_copy(c, j, i):
        return group(
            sibling, fpart.at[c, j, :, 1 - core, at(i, LEN), :], fpair.at[j, c, :, at(i, LEN), :],
            fp_send.at[j, c, i], fp_recv.at[j, c, i])

    def fr_copy(c, i, t):
        src = fpair.at[0, c, lax.rem(y + t, ny), at(i, LEN), :]
        return group(up_y(t), src, frs.at[t - 1, c, at(i, LEN), :], fr_send.at[c, i, t - 1], fr_recv.at[c, i, t - 1])

    def back(c, i):
        return pltpu.make_async_remote_copy(
            fpair.at[1, c, :, at(i, LEN), :], fpair.at[0, c, :, at(i, LEN), :], back_send.at[c, i], back_recv.at[c, i],
            device_id={"fs": partner}, device_id_type=MESH)

    def send_at(k):
        @pl.when(k == 2)
        def _():
            send_own("mix", 2)

        @pl.when(k == 3)
        def _():
            send_own("out", 0)

        @pl.when((k >= 4) & (k < 4 + nu))
        def _():
            send_own("up", k - 4)

        @pl.when((k >= 4 + nu) & (k < 4 + nu + nc))
        def _():
            send_own("down", k - 4 - nu)

    def relay_at(k, first, last, mid, out):
        @pl.when(k < 3)
        def _():
            relay("mix", k, first, last, mid, out)

        @pl.when(k == 3)
        def _():
            relay("out", 0, first, last, mid, out)

        @pl.when((k >= 4) & (k < 4 + nu))
        def _():
            relay("up", k - 4, first, last, mid, out)

        @pl.when((k >= 4 + nu) & (k < nk))
        def _():
            relay("down", k - 4 - nu, first, last, mid, out)

    def take(q):
        @pl.when(lax.rem(q, 2) == 1)
        def _():
            relay_at((q + 1) // 2, 1, 2, True, False)

        @pl.when(lax.rem(q, 2) == 0)
        def _():
            relay_at(q // 2, 1, 2, q == 0, True)
            send_at(q // 2 + 2 + jnp.where(q >= 8, 1, 0))

            @pl.when(q == 6)
            def _():
                send_at(6)

            @pl.when(q >= 2)
            def _():
                relay_at(q // 2 - 1, 2, nfs, True, True)

    def takes(low, high):
        @pl.when(worker)
        def _():
            with jax.named_scope("take"):
                loop(low, high, take)

    def outer_mix(*parts):
        @pl.when(jnp.logical_not(worker))
        def _():
            for d, k in parts:
                kind, j = ("mix", k) if k < 3 else ("out", 0)
                with jax.named_scope("relay"):
                    relay(kind, j, d, d + 1 if d < 3 else nfs)

    def send_outer(low, high):
        @pl.when(jnp.logical_not(worker))
        def _():
            loop(4 + low, 4 + min(high, nu + nc), send_at)

    def fs_copy(c, i, t):
        src = fpair.at[1, c, lax.rem(y + t, ny), at(i, LEN), :]
        dst = fsum.at[t - 1, c - n_early, at(i, LEN), :]
        return group(up_y(t), src, dst, fs_send.at[c, i, t - 1], fs_recv.at[c, i, t - 1])

    def back_own(c, i):
        return pltpu.make_async_remote_copy(
            fpair.at[1, c, y, at(i, LEN), :], fpair.at[0, c, y, at(i, LEN), :], back_send.at[c, i], back_recv.at[c, i],
            device_id={"fs": partner}, device_id_type=MESH)

    send_own("mix", 0)
    loop(0, seqs, lambda i: ag_start(2, i))
    own_tok = pltpu.make_async_copy(tokens, big.at[1, :, at(tp, own)], tok_local)
    own_tok.start()
    send_own("mix", 1)

    @pl.when(jnp.logical_not(worker))
    def _():
        send_own("mix", 2)
        send_own("out", 0)

    for k in range(3):
        local("mix", k).start()
    local("out", 0).start()

    @pl.when(worker)
    def _():
        loop(0, nu, lambda j: local("up", j).start())
        loop(0, nc, lambda j: local("down", j).start())

    takes(0, 3)
    outer_mix((1, 0), (1, 1), (2, 0), (1, 2))
    takes(3, 4)
    with jax.named_scope("tok_pass"):
        loop(0, seqs, lambda i: ag_pass(2, i))
    takes(4, 5)
    outer_mix((2, 1), (3, 0), (1, 3))
    send_outer(0, 2)
    own_tok.wait()

    def norm_tokens(i):
        ag_finish(2, i)
        r = at(i, LEN)
        v = big[1, r, :].astype(F32)
        factor = lax.rsqrt(jnp.mean(v * v, axis=-1, keepdims=True) + epsilon)
        big[0, r, :] = (v * factor * row(gain1[...])).astype(BF16)

    with jax.named_scope("norm"):
        loop(0, seqs, norm_tokens)
    takes(5, 7)
    outer_mix((2, 2), (3, 1), (2, 3))
    send_outer(2, nu)
    outer_mix((3, 2), (3, 3))
    send_outer(nu, nu + nc)
    with jax.named_scope("mix_wait"):
        for k in range(3):
            complete("mix", k)

    own_taps = taps[:, at(tp, chan)].astype(F32)
    position = lax.broadcasted_iota(jnp.int32, (LEN, chan), 0)

    def mixer(i):
        r = at(i, LEN)
        rows = big[0, r, :]
        inner = dot(rows, rows_w[1]).astype(BF16).astype(F32) * dot(rows, rows_w[2]).astype(BF16).astype(F32)
        before = jnp.where(position == 0, 0.0, pltpu.roll(inner, 1, 0))
        after = jnp.where(position == LEN - 1, 0.0, pltpu.roll(inner, LEN - 1, 0))
        conv = own_taps[0:1] * before + own_taps[1:2] * inner + own_taps[2:3] * after
        outer = dot(rows, rows_w[0]).astype(BF16).astype(F32)
        active[0, r, 0:chan] = (outer * conv).astype(BF16)

        @pl.when(i == seqs // 2)
        def _():
            takes(8, 9)

    with jax.named_scope("mixer"):
        loop(0, seqs, mixer)
    takes(7, 8)
    takes(9, 10)
    with jax.named_scope("out_wait"):
        complete("out", 0)

    def project(i):
        r = at(i, LEN)

        @pl.when(i < seqs)
        def _():
            active[1, r, 0:width] = dot(active[0, r, 0:chan], out_w[...]).astype(BF16)
            for b in range(ny):
                pair_copy(i, b).start()

        @pl.when(i > 0)
        def _():
            last = i - 1
            r = at(last, LEN)
            for b in range(ny):
                pair_copy(last, b).wait_recv()
                total = active[1, r, at(2 * b + core, own)].astype(F32) + pair[b, r, :].astype(F32)
                pair[b, r, :] = total.astype(BF16)
            for t in range(1, ny):
                rs_copy(last, t).start()

    with jax.named_scope("project"):
        loop(0, seqs + 1, project)
    takes(10, 11)
    loop(0, seqs, lambda i: ag_drain(2, i))

    own_gain2 = row(gain2[at(tp, own)])
    own_gain3 = row(gain3[at(tp, own)])

    def mixed_sum(i):
        r = at(i, LEN)
        total = pair[y, r, :].astype(F32)
        for t in range(1, ny):
            rs_copy(i, t).wait_recv()
            total = total + rs[t - 1, r, :].astype(F32)
        acc[r, :] = total
        en_put(0, i, total)

    def add_resid(i):
        r = at(i, LEN)
        scale = en_get(0, i)
        res = (big[1, r, at(tp, own)].astype(F32) + acc[r, :] * scale * own_gain2).astype(BF16)
        resid[r, :] = res
        en_put(1, i, res.astype(F32))

    def normalise(i):
        r = at(i, LEN)
        rows = (resid[r, :].astype(F32) * en_get(1, i) * own_gain3).astype(BF16)

        @pl.when(worker)
        def _():
            big[0, r, at(tp, own)] = rows
            ag_start(0, i)

        @pl.when(jnp.logical_not(worker))
        def _():
            land[r, :] = rows
            hand(i).start()

    def lift(j, i):
        ag_finish(j, i)
        r = at(i, LEN)
        rows = big[j, r, :]
        for u in range(nu):
            lifted = jnp.maximum(dot(rows, rows_w[3 + u]), 0.0)
            active[j, r, pl.ds(u * ucol, ucol)] = (lifted * lifted).astype(BF16)

    def exchange(step):
        @pl.when(step <= seqs)
        def _():
            takes(11 + step, 12 + step)

        @pl.when(step < seqs)
        def _():
            with jax.named_scope("mixed_sum"):
                mixed_sum(step)
            for b in range(ny):
                pair_copy(step, b).wait_send()

        @pl.when((step >= seqs) & (step < 2 * seqs))
        def _():
            with jax.named_scope("add_resid"):
                add_resid(step - seqs)

        @pl.when(step >= 2 * seqs)
        def _():
            with jax.named_scope("normalise"):
                normalise(step - 2 * seqs)

        @pl.when(step < 3)
        def _():
            drain("mix", step)

    def spread(step):
        takes(taken + step, taken + step + 1)

        @pl.when(step < seqs)
        def _():
            with jax.named_scope("ag_pass0"):
                ag_pass(0, step)

        @pl.when(step == 1)
        def _():
            with jax.named_scope("up_wait"):
                loop(0, nu, lambda j: complete("up", j))

        @pl.when(step >= 1)
        def _():
            with jax.named_scope("lift0"):
                lift(0, step - 1)

    loop(0, 3 * seqs, exchange)
    taken = 12 + seqs
    drain("out", 0)

    @pl.when(worker)
    def _():
        loop(0, seqs + 1, spread)

    taken += seqs + 1

    def sum_pair(c, j, i):
        r = at(i, LEN)
        fp_copy(c, j, i).wait_recv()
        for b in range(ny):
            total = fpart[c, j, b, core, r, :].astype(F32) + fpair[j, c, b, r, :].astype(F32)
            fpair[j, c, b, r, :] = total.astype(BF16)

    def fr_start(c, i):
        for t in range(1, ny):
            fr_copy(c, i, t).start()

    @pl.when(jnp.logical_not(worker))
    def _():
        loop(0, nu, lambda j: drain("up", j))

        frs[:, n_early:] = jnp.zeros((ny - 1, nc - n_early, count, piece), BF16)

        def returned(c):
            def one(i):
                back(c, i).wait_recv()
                fr_start(c, i)

            loop(0, seqs, one)

        with jax.named_scope("returned"):
            loop(0, n_early, returned)

    @pl.when(worker)
    def _():
        lag = 2
        total = 2 * nk + 1

        def unit(c, j, i):
            r = at(i, LEN)
            product = dot(active[j, r, 0:hidden], down_w[c]).astype(BF16)
            for b in range(ny):
                for odd_ in range(2):
                    lane = (2 * b + odd_) * piece
                    fpart[c, j, b, odd_, r, :] = product[:, lane:lane + piece]
            fp_copy(c, j, i).start()

        def post(c, j, i, go=True):
            sum_pair(c, j, i)

            @pl.when((j == 0) & go)
            def _():
                fr_start(c, i)

            @pl.when((j == 1) & (c < n_early))
            def _():
                back(c, i).start()

            @pl.when((j == 1) & (c >= n_early))
            def _():
                for t in range(1, ny):
                    fs_copy(c, i, t).start()

        def units(c, j, go=True):
            def one(n):
                @pl.when(n < seqs)
                def _():
                    unit(c, j, n)

                @pl.when(n >= lag)
                def _():
                    post(c, j, n - lag, go)

            with jax.named_scope("units"):
                loop(0, seqs + lag, one)

        def chunk(c):
            with jax.named_scope("down_wait"):
                complete("down", c)

        def client(step):
            @pl.when(step < seqs)
            def _():
                with jax.named_scope("hand_wait"):
                    hand(step).wait_recv()
                r = at(step, LEN)
                big[1, r, at(tp, own)] = land[r, :]
                ag_start(1, step)

            @pl.when(step < n_early)
            def _():
                chunk(step)
                units(step, 0, False)

            @pl.when((step >= 1) & (step < seqs + 1))
            def _():
                with jax.named_scope("ag_pass1"):
                    ag_pass(1, step - 1)

            takes(reached + 2 * step, jnp.minimum(reached + 2 * step + 2, total))

            @pl.when(step == seqs)
            def _():
                loop(0, n_early, lambda c: loop(0, seqs, lambda i: fr_start(c, i)))

            @pl.when(step >= 2)
            def _():
                i = step - 2
                with jax.named_scope("lift1"):
                    lift(1, i)
                with jax.named_scope("early"):
                    loop(0, n_early, lambda c: unit(c, 1, i))
                    loop(0, n_early, lambda c: post(c, 1, i))

        reached = max(taken, 2 * (4 + nu + n_early - 1) + 3) if nc > 1 else taken
        takes(taken, reached)
        loop(0, seqs + 2, client)
        takes(min(reached + 2 * (seqs + 2), total), total)

        def gather(c, i):
            r = at(i, LEN)
            sums = fpair[1, c, y, r, :].astype(F32)
            for t in range(1, ny):
                fs_copy(c, i, t).wait_recv()
                sums = sums + fsum[t - 1, c - n_early, r, :].astype(F32)
            fpair[1, c, y, r, :] = sums.astype(BF16)
            back_own(c, i).start()

        def later(c):
            chunk(c)
            units(c, 1)

            @pl.when(c > n_early)
            def _():
                with jax.named_scope("gather"):
                    loop(0, seqs, lambda i: gather(c - 1, i))

        loop(n_early, nc, later)
        units(n_early, 0)
        with jax.named_scope("gather"):
            loop(0, seqs, lambda i: gather(nc - 1, i))
        loop(n_early + 1, nc, lambda c: units(c, 0))
        loop(0, nu, lambda j: drain("up", j))

    own_gain4 = row(gain4[at(tp, own)])

    def close(step):
        @pl.when(step < seqs)
        def _():
            r = at(step, LEN)
            parts = []
            for c in range(nc):
                if c >= n_early:
                    @pl.when(jnp.logical_not(worker))
                    def _():
                        back_own(c, step).wait_recv()
                total = fpair[0, c, y, r, :].astype(F32)
                for t in range(1, ny):
                    @pl.when(worker | (c < n_early))
                    def _():
                        fr_copy(c, step, t).wait_recv()
                    total = total + frs[t - 1, c, r, :].astype(F32)
                parts.append(total)
            total = parts[0] if nc == 1 else jnp.concatenate(parts, axis=1)
            acc[r, :] = total
            en_put(2, step, total)

        @pl.when(step > 0)
        def _():
            r = at(step - 1, LEN)
            scale = en_get(2, step - 1)
            result[r, :] = (resid[r, :].astype(F32) + acc[r, :] * scale * own_gain4).astype(BF16)

    with jax.named_scope("close"):
        loop(0, seqs + 1, close)

    with jax.named_scope("drain"):
        loop(0, nc, lambda j: drain("down", j))

    def finish(i):
        for t in range(1, ny):
            rs_copy(i, t).wait_send()
            loop(0, jnp.where(worker, nc, n_early), lambda c: fr_copy(c, i, t).wait_send())
        for stage in range(3):
            for t in range(1, ntp):
                en_copy(stage, i, t).wait_send()

        @pl.when(worker)
        def _():
            ag_drain(0, i)
            ag_drain(1, i)
            for j in range(2):
                loop(0, nc, lambda c: fp_copy(c, j, i).wait_send())
            loop(0, n_early, lambda c: back(c, i).wait_send())
            loop(n_early, nc, lambda c: back_own(c, i).wait_send())
            for t in range(1, ny):
                loop(n_early, nc, lambda c: fs_copy(c, i, t).wait_send())

        @pl.when(jnp.logical_not(worker))
        def _():
            hand(i).wait_send()

    with jax.named_scope("finish"):
        loop(0, seqs, finish)


def solution(mesh):
    nfs, ntp = mesh.shape["fs"], mesh.shape["tp"]
    assert mesh.shape["rep"] == 2 and nfs % 2 == 0 and nfs >= 4 and ntp % 2 == 0

    def body(tokens, gain1, wb, wc, wv, taps, wo, gain2, gain3, wu, wd, gain4):
        count, own = tokens.shape
        width, chan, hidden = own * ntp, wb.shape[1], wu.shape[1]
        nu = hidden // chan
        cw = min(LANES, wd.shape[1])
        nc = wd.shape[1] // cw
        nk = 4 + nu + nc
        ny, seqs = ntp // 2, count // LEN
        piece = nfs * cw // ntp
        vm, anyw = pl.BlockSpec(memory_space=pltpu.VMEM), pl.BlockSpec(memory_space=pl.ANY)
        dma = pltpu.SemaphoreType.DMA
        return pl.pallas_call(
            functools.partial(kernel, nfs, ntp, nu, nc, cw),
            out_shape=jax.ShapeDtypeStruct((count, own), BF16),
            in_specs=[anyw, vm, anyw, anyw, anyw, vm, anyw, vm, vm, anyw, anyw, vm],
            out_specs=vm,
            scratch_shapes=[
                pltpu.VMEM((3 + nu, width, chan), BF16),
                pltpu.VMEM((chan, width), BF16),
                pltpu.VMEM((nc, hidden, nfs * cw), BF16),
                pltpu.VMEM((2, count, width), BF16),
                pltpu.VMEM((2, count, max(hidden, width)), BF16),
                pltpu.VMEM((count, own), BF16),
                pltpu.VMEM((ny, count, own), BF16),
                pltpu.VMEM((ny - 1, count, own), BF16),
                pltpu.VMEM((count, own), F32),
                pltpu.VMEM((count, own), BF16),
                pltpu.VMEM((nc, 2, ny, 2, count, piece), BF16),
                pltpu.VMEM((2, nc, ny, count, piece), BF16),
                pltpu.VMEM((ny - 1, nc, count, piece), BF16),
                pltpu.VMEM((ny - 1, nc - early_chunks(nc), count, piece), BF16),
                pltpu.VMEM((3, ntp, seqs, 8, LEN), F32),
                dma((nk, nfs)), dma((nk, nfs)), dma((nk, nfs)), dma((nk, nfs)), dma((nk, nfs)),
                dma((nk,)), dma,
                dma((3, seqs, ny - 1)), dma((3, seqs, ny)), dma((3, seqs, ntp)), dma((seqs,)), dma((seqs,)),
                dma((seqs, ny)), dma((seqs, ny)), dma((seqs, ny - 1)), dma((seqs, ny - 1)),
                dma((3, seqs, ntp - 1)), dma((3, seqs, ntp - 1)),
                dma((2, nc, seqs)), dma((2, nc, seqs)), dma((nc, seqs, ny - 1)), dma((nc, seqs, ny - 1)),
                dma((nc, seqs)), dma((nc, seqs)), dma((nc, seqs, ny - 1)), dma((nc, seqs, ny - 1)),
            ],
            compiler_params=pltpu.CompilerParams(
                collective_id=0, has_side_effects=True, vmem_limit_bytes=67043328),
            name="layer",
        )(tokens, gain1, wb, wc, wv, taps, wo, gain2, gain3, wu, wd, gain4)

    placed = (
        P(("rep", "fs"), "tp"), P(), P("fs", "tp"), P("fs", "tp"), P("fs", "tp"), P(), P("tp", "fs"),
        P(), P(), P("fs", "tp"), P("tp", "fs"), P(),
    )
    return jax.shard_map(
        body, mesh=mesh, in_specs=placed, out_specs=P(("rep", "fs"), "tp"), check_vma=False
    )
```

```python
import functools

import jax
import jax.numpy as jnp
from jax import lax
from jax.experimental import pallas as pl
from jax.experimental.pallas import tpu as pltpu
from jax.sharding import PartitionSpec as P

LEN = 256
LANES = 128
DOWN_BOTH = 2

epsilon = 1e-06
MESH = pl.DeviceIdType.MESH
F32 = jnp.float32
BF16 = jnp.bfloat16


def at(index, size):
    return pl.ds(pl.multiple_of(index * size, size), size)


def dot(left, right):
    return jnp.dot(left, right, preferred_element_type=F32)


def row(v):
    return v.astype(F32).reshape(1, v.shape[0])


def early_chunks(nc):
    return min(2, nc - 1)


def loop(low, high, fn):
    def one(i, carry):
        fn(i)
        return carry

    lax.fori_loop(low, high, one, 0)


def kernel(
    nfs, ntp, nu, nc, cw,
    tokens, gain1, wb, wc, wv, taps, wo, gain2, gain3, wu, wd, gain4,
    result,
    rows_w, out_w, down_w, big, active, land, pair, rs, acc, resid, fpart, fpair, frs, fsum, energy,
    recv_z, recv_x, send_r, send_l, send_x, local_sem, tok_local,
    ag_send, ag_recv, land_send, land_recv,
    pair_send, pair_recv, rs_send, rs_recv, en_send, en_recv,
    fp_send, fp_recv, fr_send, fr_recv, back_send, back_recv, fs_send, fs_recv,
):
    rep, fs, tp = lax.axis_index("rep"), lax.axis_index("fs"), lax.axis_index("tp")
    ny = ntp // 2
    core, y = lax.rem(tp, 2), tp // 2
    sibling = tp + 1 - 2 * core
    count, own = tokens.shape
    width = own * ntp
    seqs = count // LEN
    krows, chan = wb.shape
    hidden = wu.shape[1]
    ucol = hidden // nu
    ocol = wo.shape[1]
    nk = 4 + nu + nc
    n_early = early_chunks(nc)
    late = 4 + nu + min(2, nc)
    block = nfs * cw
    piece = block // ntp
    odd = lax.rem(fs, 2)
    worker = jnp.where(fs < nfs // 2, odd, 1 - odd) == 1
    partner = fs + 1 - 2 * odd
    end = (fs == 0) | (fs == nfs - 1)

    barrier = pltpu.get_barrier_semaphore()
    for step in (1, nfs - 1):
        pl.semaphore_signal(barrier, inc=1, device_id={"fs": lax.rem(fs + step, nfs)}, device_id_type=MESH)
    pl.semaphore_signal(barrier, inc=1, device_id={"rep": 1 - rep}, device_id_type=MESH)
    for step in range(1, ntp):
        pl.semaphore_signal(barrier, inc=1, device_id={"tp": lax.rem(tp + step, ntp)}, device_id_type=MESH)
    pl.semaphore_wait(barrier, 3 + ntp - 1)

    def slot(kind, j):
        return {"mix": j, "out": 3, "up": 4 + j, "down": 4 + nu + j}[kind]

    def ends(kind):
        return (0, nfs - 1) if kind in ("mix", "out") else (1, nfs - 2)

    def region(kind, j, s, half):
        if kind in ("mix", "up"):
            index = j if kind == "mix" else 3 + j
            if half is None:
                return rows_w.at[index, at(s, krows), :]
            return rows_w.at[index, at(s * 2 + half, krows // 2), :]
        if kind == "out":
            r = slice(None) if half is None else at(half, wo.shape[0] // 2)
            return out_w.at[r, at(s, ocol)]
        r = slice(None) if half is None else at(half, wd.shape[0] // 2)
        return down_w.at[j, r, at(s, cw)]

    def source(kind, j, half):
        if kind == "mix":
            ref, c = (wb, wc, wv)[j], slice(None)
        elif kind == "out":
            ref, c = wo, slice(None)
        elif kind == "up":
            ref, c = wu, at(j, ucol)
        else:
            ref, c = wd, at(j, cw)
        r = slice(None) if half is None else at(half, ref.shape[0] // 2)
        return ref.at[r, c]

    def hop(kind, j, s, mine, sems, to):
        k = slot(kind, j)
        src = source(kind, j, rep) if mine else region(kind, j, s, rep)
        return pltpu.make_async_remote_copy(
            src, region(kind, j, s, rep), sems.at[k, s], recv_z.at[k, s],
            device_id={"fs": to}, device_id_type=MESH)

    def right(kind, j, s, mine=False):
        return hop(kind, j, s, mine, send_r, lax.rem(fs + 1, nfs))

    def left(kind, j, s, mine=False):
        return hop(kind, j, s, mine, send_l, lax.rem(fs + nfs - 1, nfs))

    def across(kind, j, s, half):
        k = slot(kind, j)
        return pltpu.make_async_remote_copy(
            region(kind, j, s, half), region(kind, j, s, half), send_x.at[k, s], recv_x.at[k, s],
            device_id={"rep": 1 - rep}, device_id_type=MESH)

    def extra(kind, j, src):
        k = slot(kind, j)
        to = jnp.where(fs == 0, 1, nfs - 2)
        return pltpu.make_async_remote_copy(
            src, region(kind, j, fs, 1 - rep), send_x.at[k, fs], recv_x.at[k, fs],
            device_id={"fs": to}, device_id_type=MESH)

    def both(kind, j):
        return j < DOWN_BOTH if kind == "down" else True

    def crosses(kind, j, s):
        near = ((s == 0) & (fs == 1)) | ((s == nfs - 1) & (fs == nfs - 2))
        keep = jnp.logical_not(near & both(kind, j)) & (s != fs)
        return keep if kind in ("mix", "out") else keep & worker

    def send_own(kind, j):
        low, high = ends(kind)

        @pl.when(fs < high)
        def _():
            right(kind, j, fs, True).start()

        @pl.when(fs > low)
        def _():
            left(kind, j, fs, True).start()

        @pl.when(end & both(kind, j))
        def _():
            extra(kind, j, source(kind, j, 1 - rep)).start()

    def local(kind, j):
        return pltpu.make_async_copy(source(kind, j, None), region(kind, j, fs, None), local_sem.at[slot(kind, j)])

    def relay(kind, j, first, last, mid=True, out=True):
        low, high = ends(kind)
        inside = (fs >= low) & (fs <= high)
        lower = fs < nfs // 2
        from_left = inside & ((lower & out) | (jnp.logical_not(lower) & mid))
        from_right = inside & ((lower & mid) | (jnp.logical_not(lower) & out))

        def one(d):
            @pl.when((fs - d >= 0) & from_left)
            def _():
                s = fs - d
                right(kind, j, s).wait_recv()

                @pl.when(fs < high)
                def _():
                    right(kind, j, s).start()

                @pl.when(crosses(kind, j, s))
                def _():
                    across(kind, j, s, rep).start()

            @pl.when((fs + d < nfs) & from_right)
            def _():
                s = fs + d
                left(kind, j, s).wait_recv()

                @pl.when(fs > low)
                def _():
                    left(kind, j, s).start()

                @pl.when(crosses(kind, j, s))
                def _():
                    across(kind, j, s, rep).start()

        loop(first, last, one)

    def complete(kind, j):
        def one(s):
            @pl.when(s != fs)
            def _():
                across(kind, j, s, 1 - rep).wait_recv()

        loop(0, nfs, one)
        local(kind, j).wait()

    def drain(kind, j):
        low, high = ends(kind)

        def one(s):
            @pl.when((s <= fs) & (fs < high))
            def _():
                right(kind, j, s).wait_send()

            @pl.when((s >= fs) & (fs > low))
            def _():
                left(kind, j, s).wait_send()

            inside = (fs >= low) & (fs <= high)

            @pl.when(crosses(kind, j, s) & inside)
            def _():
                across(kind, j, s, rep).wait_send()

        loop(0, nfs, one)

        @pl.when(end & both(kind, j))
        def _():
            extra(kind, j, region(kind, j, fs, 1 - rep)).wait_send()

    def group(to, src, dst, send, recv):
        return pltpu.make_async_remote_copy(
            src, dst, send, recv, device_id={"tp": to}, device_id_type=MESH)

    def up_y(t):
        return lax.rem(y + t, ny) * 2 + core

    def down_y(t):
        return lax.rem(y + ny - t, ny) * 2 + core

    def gathered(j, i, who):
        return big.at[min(j, 1), at(i, LEN), at(who, own)]

    def ag_y(j, i, t):
        src = tokens.at[at(i, LEN), :] if j == 2 else gathered(j, i, tp)
        return group(up_y(t), src, gathered(j, i, tp), ag_send.at[j], ag_recv.at[j, i, tp])

    def ag_pair(j, i):
        src = tokens.at[at(i, LEN), :] if j == 2 else gathered(j, i, tp)
        return group(sibling, src, gathered(j, i, tp), ag_send.at[j], ag_recv.at[j, i, tp])

    def ag_relay(j, i, t):
        who = down_y(t)
        return group(sibling, gathered(j, i, who), gathered(j, i, who), ag_send.at[j], ag_recv.at[j, i, who])

    def ag_start(j, i):
        for t in range(1, ny):
            ag_y(j, i, t).start()
        ag_pair(j, i).start()

    def ag_pass(j, i):
        for t in range(1, ny):
            ag_relay(j, i, t).wait_recv()
            ag_relay(j, i, t).start()

    def ag_finish(j, i):
        for t in range(ny):
            who = lax.rem(y + t, ny) * 2 + 1 - core
            group(sibling, gathered(j, i, who), gathered(j, i, who), ag_send.at[j], ag_recv.at[j, i, who]).wait_recv()

    def ag_drain(j):
        sent = big.at[min(j, 1), :, 0:(2 * ny - 1) * own]
        group(sibling, sent, sent, ag_send.at[j], ag_recv.at[j, 0, tp]).wait_send()

    def hand(i):
        return pltpu.make_async_remote_copy(
            land.at[at(i, LEN), :], land.at[at(i, LEN), :], land_send.at[i], land_recv.at[i],
            device_id={"fs": partner}, device_id_type=MESH)

    def pair_copy(i, b):
        src = active.at[1, at(i, LEN), at(2 * b + 1 - core, own)]
        return group(sibling, src, pair.at[b, at(i, LEN), :], pair_send, pair_recv.at[i, b])

    def rs_copy(i, t):
        src = pair.at[lax.rem(y + t, ny), at(i, LEN), :]
        return group(up_y(t), src, rs.at[t - 1, at(i, LEN), :], rs_send, rs_recv.at[i, t - 1])

    def en_copy(stage, i, t):
        return group(
            lax.rem(tp + t, ntp), energy.at[stage, 0, i], energy.at[stage, t, i],
            en_send, en_recv.at[stage, i])

    def en_put(stage, i, values):
        square = jnp.sum(values * values, axis=1, keepdims=True)
        flat = jnp.transpose(jnp.broadcast_to(square, (LEN, LANES)))
        energy[stage, 0, i] = flat[0:8, :]
        for t in range(1, ntp):
            en_copy(stage, i, t).start()

    def en_get(stage, i):
        others = energy.at[stage, 1:ntp, i]
        group(sibling, others, others, en_send, en_recv.at[stage, i]).wait_recv()
        flat = energy[stage, 0, i]
        for t in range(1, ntp):
            flat = flat + energy[stage, t, i]
        tall = jnp.transpose(jnp.concatenate([flat] * (LANES // 8), axis=0))
        return lax.rsqrt(tall[:, 0:1] / width + epsilon)

    def fp_copy(c, j, i):
        return group(
            sibling, fpart.at[c, j, :, 1 - core, at(i, LEN), :], fpair.at[j, c, :, at(i, LEN), :],
            fp_send, fp_recv.at[j, c, i])

    def fr_copy(c, i, t):
        src = fpair.at[0, c, lax.rem(y + t, ny), at(i, LEN), :]
        return group(up_y(t), src, frs.at[t - 1, c, at(i, LEN), :], fr_send, fr_recv.at[c, i, t - 1])

    def back(c, i):
        return pltpu.make_async_remote_copy(
            fpair.at[1, c, :, at(i, LEN), :], fpair.at[0, c, :, at(i, LEN), :], back_send.at[0], back_recv.at[c, i],
            device_id={"fs": partner}, device_id_type=MESH)

    def send_at(k):
        @pl.when(k == 2)
        def _():
            send_own("mix", 2)

        @pl.when(k == 3)
        def _():
            send_own("out", 0)

        @pl.when((k >= 4) & (k < 4 + nu))
        def _():
            send_own("up", k - 4)

        @pl.when((k >= 4 + nu) & (k < 4 + nu + nc))
        def _():
            send_own("down", k - 4 - nu)

    def relay_at(k, first, last, mid, out):
        @pl.when(k < 3)
        def _():
            relay("mix", k, first, last, mid, out)

        @pl.when(k == 3)
        def _():
            relay("out", 0, first, last, mid, out)

        @pl.when((k >= 4) & (k < 4 + nu))
        def _():
            relay("up", k - 4, first, last, mid, out)

        @pl.when((k >= 4 + nu) & (k < nk))
        def _():
            relay("down", k - 4 - nu, first, last, mid, out)

    def take(q):
        @pl.when(lax.rem(q, 2) == 1)
        def _():
            relay_at((q + 1) // 2, 1, 2, True, False)

        @pl.when(lax.rem(q, 2) == 0)
        def _():
            @pl.when(q // 2 < late)
            def _():
                relay_at(q // 2, 1, 2, q == 0, True)

            send_at(q // 2 + 2 + jnp.where(q >= 8, 1, 0))

            @pl.when(q == 6)
            def _():
                send_at(6)

            @pl.when((q >= 2) & (q // 2 - 1 < late))
            def _():
                relay_at(q // 2 - 1, 2, nfs, True, True)

    def takes(low, high):
        @pl.when(worker)
        def _():
            with jax.named_scope("take"):
                loop(low, high, take)

    def outer_mix(*parts):
        @pl.when(jnp.logical_not(worker))
        def _():
            for d, k in parts:
                kind, j = ("mix", k) if k < 3 else ("out", 0)
                with jax.named_scope("relay"):
                    relay(kind, j, d, d + 1 if d < 3 else nfs)

    def send_outer(low, high):
        @pl.when(jnp.logical_not(worker))
        def _():
            loop(4 + low, 4 + min(high, nu + nc), send_at)

    def fs_copy(c, i, t):
        src = fpair.at[1, c, lax.rem(y + t, ny), at(i, LEN), :]
        dst = fsum.at[t - 1, c - n_early, at(i, LEN), :]
        return group(up_y(t), src, dst, fs_send, fs_recv.at[c, i, t - 1])

    def back_own(c, i):
        return pltpu.make_async_remote_copy(
            fpair.at[1, c, y, at(i, LEN), :], fpair.at[0, c, y, at(i, LEN), :], back_send.at[1], back_recv.at[c, i],
            device_id={"fs": partner}, device_id_type=MESH)

    send_own("mix", 0)
    loop(0, seqs, lambda i: ag_start(2, i))
    own_tok = pltpu.make_async_copy(tokens, big.at[1, :, at(tp, own)], tok_local)
    own_tok.start()
    send_own("mix", 1)

    @pl.when(jnp.logical_not(worker))
    def _():
        send_own("mix", 2)
        send_own("out", 0)

    for k in range(3):
        local("mix", k).start()
    local("out", 0).start()

    @pl.when(worker)
    def _():
        loop(0, nu, lambda j: local("up", j).start())
        loop(0, nc, lambda j: local("down", j).start())

    takes(0, 3)
    outer_mix((1, 0), (1, 1), (2, 0), (1, 2))
    takes(3, 4)
    with jax.named_scope("tok_pass"):
        loop(0, seqs, lambda i: ag_pass(2, i))
    takes(4, 5)
    outer_mix((2, 1), (3, 0), (1, 3))
    send_outer(0, 2)
    own_tok.wait()

    def norm_tokens(i):
        ag_finish(2, i)
        r = at(i, LEN)
        v = big[1, r, :].astype(F32)
        factor = lax.rsqrt(jnp.mean(v * v, axis=-1, keepdims=True) + epsilon)
        big[0, r, :] = (v * factor * row(gain1[...])).astype(BF16)

    with jax.named_scope("norm"):
        loop(0, seqs, norm_tokens)
    takes(5, 7)
    outer_mix((2, 2), (3, 1), (2, 3))
    send_outer(2, nu)
    outer_mix((3, 2), (3, 3))
    send_outer(nu, nu + min(2, nc))
    with jax.named_scope("mix_wait"):
        for k in range(3):
            complete("mix", k)

    own_taps = taps[:, at(tp, chan)].astype(F32)
    position = lax.broadcasted_iota(jnp.int32, (LEN, chan), 0)

    def mixer(i):
        r = at(i, LEN)
        rows = big[0, r, :]
        inner = dot(rows, rows_w[1]).astype(BF16).astype(F32) * dot(rows, rows_w[2]).astype(BF16).astype(F32)
        before = jnp.where(position == 0, 0.0, pltpu.roll(inner, 1, 0))
        after = jnp.where(position == LEN - 1, 0.0, pltpu.roll(inner, LEN - 1, 0))
        conv = own_taps[0:1] * before + own_taps[1:2] * inner + own_taps[2:3] * after
        outer = dot(rows, rows_w[0]).astype(BF16).astype(F32)
        active[0, r, 0:chan] = (outer * conv).astype(BF16)

    def project(i):
        r = at(i, LEN)
        active[1, r, 0:width] = dot(active[0, r, 0:chan], out_w[...]).astype(BF16)
        for b in range(ny):
            pair_copy(i, b).start()

    def chip_sum(i):
        r = at(i, LEN)
        for b in range(ny):
            pair_copy(i, b).wait_recv()
            total = active[1, r, at(2 * b + core, own)].astype(F32) + pair[b, r, :].astype(F32)
            pair[b, r, :] = total.astype(BF16)

    def rs_start(i):
        for t in range(1, ny):
            rs_copy(i, t).start()

    def mix(step):
        @pl.when(step < seqs)
        def _():
            with jax.named_scope("mixer"):
                mixer(step)

        @pl.when(step == 1)
        def _():
            takes(8, 9)

        @pl.when(step == 2)
        def _():
            takes(7, 8)
            takes(9, 10)
            with jax.named_scope("out_wait"):
                complete("out", 0)

        @pl.when((step >= 2) & (step < seqs + 2))
        def _():
            with jax.named_scope("project"):
                project(step - 2)

        @pl.when(step >= 3)
        def _():
            with jax.named_scope("chip_sum"):
                chip_sum(step - 3)

        @pl.when((step == 3) | (step == 4))
        def _():
            rs_start(step - 3)

    loop(0, seqs + 3, mix)
    takes(10, 11)
    ag_drain(2)
    group(sibling, active.at[1, :, 0:ny * own], active.at[1, :, 0:ny * own], pair_send, pair_recv.at[0, 0]).wait_send()

    own_gain2 = row(gain2[at(tp, own)])
    own_gain3 = row(gain3[at(tp, own)])

    def mixed_sum(i):
        r = at(i, LEN)
        total = pair[y, r, :].astype(F32)
        for t in range(1, ny):
            rs_copy(i, t).wait_recv()
            total = total + rs[t - 1, r, :].astype(F32)
        acc[r, :] = total
        en_put(0, i, total)

    def add_resid(i):
        r = at(i, LEN)
        scale = en_get(0, i)
        res = (big[1, r, at(tp, own)].astype(F32) + acc[r, :] * scale * own_gain2).astype(BF16)
        resid[r, :] = res
        en_put(1, i, res.astype(F32))

    def normalise(i):
        r = at(i, LEN)
        rows = (resid[r, :].astype(F32) * en_get(1, i) * own_gain3).astype(BF16)

        @pl.when(worker)
        def _():
            big[0, r, at(tp, own)] = rows
            ag_start(0, i)

        @pl.when(jnp.logical_not(worker))
        def _():
            land[r, :] = rows
            hand(i).start()

    def lift(j, i):
        ag_finish(j, i)
        r = at(i, LEN)
        rows = big[j, r, :]
        for u in range(nu):
            lifted = jnp.maximum(dot(rows, rows_w[3 + u]), 0.0)
            active[j, r, pl.ds(u * ucol, ucol)] = (lifted * lifted).astype(BF16)

    def exchange(step):
        takes(11 + step, 12 + step)

        @pl.when(step < seqs)
        def _():
            with jax.named_scope("mixed_sum"):
                mixed_sum(step)

        @pl.when((step >= 1) & (step < seqs + 1))
        def _():
            with jax.named_scope("add_resid"):
                add_resid(step - 1)

        @pl.when((step >= 2) & (step < seqs + 2))
        def _():
            with jax.named_scope("normalise"):
                normalise(step - 2)

        @pl.when(step + 2 < seqs)
        def _():
            rs_start(step + 2)

        @pl.when(step < 3)
        def _():
            drain("mix", step)

    def spread(step):
        @pl.when(step < 3)
        def _():
            takes(taken + step, taken + step + 1)

        @pl.when(step < seqs)
        def _():
            with jax.named_scope("ag_pass0"):
                ag_pass(0, step)

        @pl.when(step == 1)
        def _():
            with jax.named_scope("up_wait"):
                loop(0, nu, lambda j: complete("up", j))

        @pl.when(step >= 1)
        def _():
            with jax.named_scope("lift0"):
                lift(0, step - 1)

    loop(0, max(seqs + 2, 3), exchange)
    taken = 11 + max(seqs + 2, 3)
    send_outer(nu + min(2, nc), nu + nc)
    drain("out", 0)

    @pl.when(worker)
    def _():
        loop(0, seqs + 1, spread)

    taken += min(seqs + 1, 3)

    def sum_pair(c, j, i):
        r = at(i, LEN)
        fp_copy(c, j, i).wait_recv()
        for b in range(ny):
            total = fpart[c, j, b, core, r, :].astype(F32) + fpair[j, c, b, r, :].astype(F32)
            fpair[j, c, b, r, :] = total.astype(BF16)

    def fr_start(c, i):
        for t in range(1, ny):
            fr_copy(c, i, t).start()

    @pl.when(jnp.logical_not(worker))
    def _():
        loop(0, nu, lambda j: drain("up", j))

        frs[:, n_early:] = jnp.zeros((ny - 1, nc - n_early, count, piece), BF16)

        def returned(c):
            def one(i):
                back(c, i).wait_recv()
                fr_start(c, i)

            loop(0, seqs, one)

        with jax.named_scope("returned"):
            loop(0, n_early, returned)

    @pl.when(worker)
    def _():
        lag = 2
        total = 2 * nk + 1

        def unit(c, j, i):
            r = at(i, LEN)
            product = dot(active[j, r, 0:hidden], down_w[c]).astype(BF16)
            for b in range(ny):
                for odd_ in range(2):
                    lane = (2 * b + odd_) * piece
                    fpart[c, j, b, odd_, r, :] = product[:, lane:lane + piece]
            fp_copy(c, j, i).start()

        def post(c, j, i, go=True):
            sum_pair(c, j, i)

            @pl.when((j == 0) & go)
            def _():
                fr_start(c, i)

            @pl.when((j == 1) & (c < n_early))
            def _():
                back(c, i).start()

            @pl.when((j == 1) & (c >= n_early))
            def _():
                for t in range(1, ny):
                    fs_copy(c, i, t).start()

        def units(c, j, go=True):
            def one(n):
                @pl.when(n < seqs)
                def _():
                    unit(c, j, n)

                @pl.when(n >= lag)
                def _():
                    post(c, j, n - lag, go)

            with jax.named_scope("units"):
                loop(0, seqs + lag, one)

        def chunk(c):
            with jax.named_scope("down_wait"):
                complete("down", c)

        def late_near(k):
            with jax.named_scope("late"):
                relay_at(k, 1, 2, False, True)

        def late_far(k):
            with jax.named_scope("late"):
                relay_at(k, 2, nfs, True, True)

        def client(step):
            @pl.when(step < seqs)
            def _():
                with jax.named_scope("hand_wait"):
                    hand(step).wait_recv()
                r = at(step, LEN)
                big[1, r, at(tp, own)] = land[r, :]
                ag_start(1, step)

            @pl.when((step == 0) & (n_early > 0))
            def _():
                chunk(0)
                units(0, 0, False)

            @pl.when((step >= 1) & (step < seqs + 1))
            def _():
                with jax.named_scope("ag_pass1"):
                    ag_pass(1, step - 1)

            takes(jnp.minimum(reached + step, total), jnp.minimum(reached + step + 1, total))

            @pl.when((step >= 3) & (late + step - 3 < nk))
            def _():
                late_near(late + step - 3)

            @pl.when((step >= 5) & (late + step - 5 < nk))
            def _():
                late_far(late + step - 5)

            @pl.when(step >= 2)
            def _():
                i = step - 2
                with jax.named_scope("lift1"):
                    lift(1, i)

                @pl.when(step == 2)
                def _():
                    for c in range(1, n_early):
                        chunk(c)

                @pl.when(step == seqs)
                def _():
                    if n_early > 0:
                        loop(0, seqs, lambda i: fr_start(0, i))

                with jax.named_scope("early"):
                    loop(0, n_early, lambda c: unit(c, 1, i))
                    loop(0, n_early, lambda c: post(c, 1, i))

        reached = max(taken, 2 * (4 + nu) + 2 + n_early) if nc > 1 else taken
        takes(taken, reached)
        loop(0, seqs + 2, client)
        takes(min(reached + seqs + 2, total), total)
        loop(min(late + seqs - 1, nk), nk, late_near)
        loop(min(late + seqs - 3, nk), nk, late_far)
        for c in range(1, n_early):
            units(c, 0)

        def gather(c, i):
            r = at(i, LEN)
            sums = fpair[1, c, y, r, :].astype(F32)
            for t in range(1, ny):
                fs_copy(c, i, t).wait_recv()
                sums = sums + fsum[t - 1, c - n_early, r, :].astype(F32)
            fpair[1, c, y, r, :] = sums.astype(BF16)
            back_own(c, i).start()

        def later(c):
            chunk(c)
            units(c, 1)

            @pl.when(c > n_early)
            def _():
                with jax.named_scope("gather"):
                    loop(0, seqs, lambda i: gather(c - 1, i))

        loop(n_early, nc, later)
        units(n_early, 0)
        with jax.named_scope("gather"):
            loop(0, seqs, lambda i: gather(nc - 1, i))
        loop(n_early + 1, nc, lambda c: units(c, 0))
        loop(0, nu, lambda j: drain("up", j))

    own_gain4 = row(gain4[at(tp, own)])

    def close(step):
        @pl.when(step < seqs)
        def _():
            r = at(step, LEN)
            parts = []
            for c in range(nc):
                if c >= n_early:
                    @pl.when(jnp.logical_not(worker))
                    def _():
                        back_own(c, step).wait_recv()
                total = fpair[0, c, y, r, :].astype(F32)
                for t in range(1, ny):
                    @pl.when(worker | (c < n_early))
                    def _():
                        fr_copy(c, step, t).wait_recv()
                    total = total + frs[t - 1, c, r, :].astype(F32)
                parts.append(total)
            total = parts[0] if nc == 1 else jnp.concatenate(parts, axis=1)
            acc[r, :] = total
            en_put(2, step, total)

        @pl.when(step > 0)
        def _():
            r = at(step - 1, LEN)
            scale = en_get(2, step - 1)
            result[r, :] = (resid[r, :].astype(F32) + acc[r, :] * scale * own_gain4).astype(BF16)

    with jax.named_scope("close"):
        loop(0, seqs + 1, close)

    with jax.named_scope("drain"):
        loop(0, nc, lambda j: drain("down", j))

    def sent(ref, sem):
        group(sibling, ref, ref, sem, pair_recv.at[0, 0]).wait_send()

    with jax.named_scope("finish"):
        sent(rs, rs_send)
        sent(energy.at[:, 1:ntp], en_send)

        @pl.when(worker)
        def _():
            ag_drain(0)
            ag_drain(1)
            sent(fpair, fp_send)
            sent(frs, fr_send)
            sent(fsum, fs_send)
            sent(fpair.at[1, n_early:nc, 0], back_send.at[1])
            if n_early > 0:
                sent(fpair.at[1, 0:n_early], back_send.at[0])

        @pl.when(jnp.logical_not(worker))
        def _():
            if n_early > 0:
                sent(frs.at[:, 0:n_early], fr_send)
            loop(0, seqs, lambda i: hand(i).wait_send())


def solution(mesh):
    nfs, ntp = mesh.shape["fs"], mesh.shape["tp"]
    assert mesh.shape["rep"] == 2 and nfs % 2 == 0 and nfs >= 4 and ntp % 2 == 0

    def body(tokens, gain1, wb, wc, wv, taps, wo, gain2, gain3, wu, wd, gain4):
        count, own = tokens.shape
        width, chan, hidden = own * ntp, wb.shape[1], wu.shape[1]
        nu = hidden // chan
        cw = min(LANES, wd.shape[1])
        nc = wd.shape[1] // cw
        nk = 4 + nu + nc
        ny, seqs = ntp // 2, count // LEN
        piece = nfs * cw // ntp
        vm, anyw = pl.BlockSpec(memory_space=pltpu.VMEM), pl.BlockSpec(memory_space=pl.ANY)
        dma = pltpu.SemaphoreType.DMA
        return pl.pallas_call(
            functools.partial(kernel, nfs, ntp, nu, nc, cw),
            out_shape=jax.ShapeDtypeStruct((count, own), BF16),
            in_specs=[anyw, vm, anyw, anyw, anyw, vm, anyw, vm, vm, anyw, anyw, vm],
            out_specs=vm,
            scratch_shapes=[
                pltpu.VMEM((3 + nu, width, chan), BF16),
                pltpu.VMEM((chan, width), BF16),
                pltpu.VMEM((nc, hidden, nfs * cw), BF16),
                pltpu.VMEM((2, count, width), BF16),
                pltpu.VMEM((2, count, max(hidden, width)), BF16),
                pltpu.VMEM((count, own), BF16),
                pltpu.VMEM((ny, count, own), BF16),
                pltpu.VMEM((ny - 1, count, own), BF16),
                pltpu.VMEM((count, own), F32),
                pltpu.VMEM((count, own), BF16),
                pltpu.VMEM((nc, 2, ny, 2, count, piece), BF16),
                pltpu.VMEM((2, nc, ny, count, piece), BF16),
                pltpu.VMEM((ny - 1, nc, count, piece), BF16),
                pltpu.VMEM((ny - 1, nc - early_chunks(nc), count, piece), BF16),
                pltpu.VMEM((3, ntp, seqs, 8, LEN), F32),
                dma((nk, nfs)), dma((nk, nfs)), dma((nk, nfs)), dma((nk, nfs)), dma((nk, nfs)),
                dma((nk,)), dma,
                dma((3,)), dma((3, seqs, ntp)), dma((seqs,)), dma((seqs,)),
                dma, dma((seqs, ny)), dma, dma((seqs, ny - 1)),
                dma, dma((3, seqs)),
                dma, dma((2, nc, seqs)), dma, dma((nc, seqs, ny - 1)),
                dma((2,)), dma((nc, seqs)), dma, dma((nc, seqs, ny - 1)),
            ],
            compiler_params=pltpu.CompilerParams(
                collective_id=0, has_side_effects=True, vmem_limit_bytes=67043328),
            name="layer",
        )(tokens, gain1, wb, wc, wv, taps, wo, gain2, gain3, wu, wd, gain4)

    placed = (
        P(("rep", "fs"), "tp"), P(), P("fs", "tp"), P("fs", "tp"), P("fs", "tp"), P(), P("tp", "fs"),
        P(), P(), P("fs", "tp"), P("tp", "fs"), P(),
    )
    return jax.shard_map(
        body, mesh=mesh, in_specs=placed, out_specs=P(("rep", "fs"), "tp"), check_vma=False
    )
```

```python
import functools

import jax
import jax.numpy as jnp
from jax import lax
from jax.experimental import pallas as pl
from jax.experimental.pallas import tpu as pltpu
from jax.sharding import PartitionSpec as P

LEN = 256
LANES = 128
DOWN_BOTH = 2

epsilon = 1e-06
MESH = pl.DeviceIdType.MESH
F32 = jnp.float32
BF16 = jnp.bfloat16


def at(index, size):
    return pl.ds(pl.multiple_of(index * size, size), size)


def dot(left, right):
    return jnp.dot(left, right, preferred_element_type=F32)


def row(v):
    return v.astype(F32).reshape(1, v.shape[0])


def early_chunks(nc):
    return min(2, nc - 1)


def direct_chunks(nc):
    return min(3, nc - 1)


def loop(low, high, fn):
    def one(i, carry):
        fn(i)
        return carry

    lax.fori_loop(low, high, one, 0)


def kernel(
    nfs, ntp, nu, nc, cw,
    tokens, gain1, wb, wc, wv, taps, wo, gain2, gain3, wu, wd, gain4,
    result,
    rows_w, out_w, down_w, big, active, land, pair, rs, acc, resid, fpart, fpair, frs, fsum, energy,
    recv_z, recv_x, send_r, send_l, send_x, local_sem, tok_local,
    ag_send, ag_recv, land_send, land_recv,
    pair_send, pair_recv, rs_send, rs_recv, en_send, en_recv,
    fp_send, fp_recv, fr_send, fr_recv, back_send, back_recv, fs_send, fs_recv,
):
    rep, fs, tp = lax.axis_index("rep"), lax.axis_index("fs"), lax.axis_index("tp")
    ny = ntp // 2
    core, y = lax.rem(tp, 2), tp // 2
    sibling = tp + 1 - 2 * core
    count, own = tokens.shape
    width = own * ntp
    seqs = count // LEN
    krows, chan = wb.shape
    hidden = wu.shape[1]
    ucol = hidden // nu
    ocol = wo.shape[1]
    nk = 4 + nu + nc
    n_early = early_chunks(nc)
    n_direct = direct_chunks(nc)
    late = 4 + nu + min(2, nc)
    block = nfs * cw
    piece = block // ntp
    odd = lax.rem(fs, 2)
    worker = jnp.where(fs < nfs // 2, odd, 1 - odd) == 1
    partner = fs + 1 - 2 * odd
    end = (fs == 0) | (fs == nfs - 1)

    barrier = pltpu.get_barrier_semaphore()
    for step in (1, nfs - 1):
        pl.semaphore_signal(barrier, inc=1, device_id={"fs": lax.rem(fs + step, nfs)}, device_id_type=MESH)
    pl.semaphore_signal(barrier, inc=1, device_id={"rep": 1 - rep}, device_id_type=MESH)
    for step in range(1, ntp):
        pl.semaphore_signal(barrier, inc=1, device_id={"tp": lax.rem(tp + step, ntp)}, device_id_type=MESH)
    pl.semaphore_wait(barrier, 3 + ntp - 1)

    def slot(kind, j):
        return {"mix": j, "out": 3, "up": 4 + j, "down": 4 + nu + j}[kind]

    def ends(kind):
        return (0, nfs - 1) if kind in ("mix", "out") else (1, nfs - 2)

    def region(kind, j, s, half):
        if kind in ("mix", "up"):
            index = j if kind == "mix" else 3 + j
            if half is None:
                return rows_w.at[index, at(s, krows), :]
            return rows_w.at[index, at(s * 2 + half, krows // 2), :]
        if kind == "out":
            r = slice(None) if half is None else at(half, wo.shape[0] // 2)
            return out_w.at[r, at(s, ocol)]
        r = slice(None) if half is None else at(half, wd.shape[0] // 2)
        return down_w.at[j, r, at(s, cw)]

    def source(kind, j, half):
        if kind == "mix":
            ref, c = (wb, wc, wv)[j], slice(None)
        elif kind == "out":
            ref, c = wo, slice(None)
        elif kind == "up":
            ref, c = wu, at(j, ucol)
        else:
            ref, c = wd, at(j, cw)
        r = slice(None) if half is None else at(half, ref.shape[0] // 2)
        return ref.at[r, c]

    def hop(kind, j, s, mine, sems, to):
        k = slot(kind, j)
        src = source(kind, j, rep) if mine else region(kind, j, s, rep)
        return pltpu.make_async_remote_copy(
            src, region(kind, j, s, rep), sems.at[k, s], recv_z.at[k, s],
            device_id={"fs": to}, device_id_type=MESH)

    def right(kind, j, s, mine=False):
        return hop(kind, j, s, mine, send_r, lax.rem(fs + 1, nfs))

    def left(kind, j, s, mine=False):
        return hop(kind, j, s, mine, send_l, lax.rem(fs + nfs - 1, nfs))

    def across(kind, j, s, half):
        k = slot(kind, j)
        return pltpu.make_async_remote_copy(
            region(kind, j, s, half), region(kind, j, s, half), send_x.at[k, s], recv_x.at[k, s],
            device_id={"rep": 1 - rep}, device_id_type=MESH)

    def extra(kind, j, src):
        k = slot(kind, j)
        to = jnp.where(fs == 0, 1, nfs - 2)
        return pltpu.make_async_remote_copy(
            src, region(kind, j, fs, 1 - rep), send_x.at[k, fs], recv_x.at[k, fs],
            device_id={"fs": to}, device_id_type=MESH)

    def both(kind, j):
        return j < DOWN_BOTH if kind == "down" else True

    def crosses(kind, j, s):
        near = ((s == 0) & (fs == 1)) | ((s == nfs - 1) & (fs == nfs - 2))
        keep = jnp.logical_not(near & both(kind, j)) & (s != fs)
        return keep if kind in ("mix", "out") else keep & worker

    def send_own(kind, j):
        low, high = ends(kind)

        @pl.when(fs < high)
        def _():
            right(kind, j, fs, True).start()

        @pl.when(fs > low)
        def _():
            left(kind, j, fs, True).start()

        @pl.when(end & both(kind, j))
        def _():
            extra(kind, j, source(kind, j, 1 - rep)).start()

    def local(kind, j):
        return pltpu.make_async_copy(source(kind, j, None), region(kind, j, fs, None), local_sem.at[slot(kind, j)])

    def relay(kind, j, first, last, mid=True, out=True):
        low, high = ends(kind)
        inside = (fs >= low) & (fs <= high)
        lower = fs < nfs // 2
        from_left = inside & ((lower & out) | (jnp.logical_not(lower) & mid))
        from_right = inside & ((lower & mid) | (jnp.logical_not(lower) & out))

        def one(d):
            @pl.when((fs - d >= 0) & from_left)
            def _():
                s = fs - d
                right(kind, j, s).wait_recv()

                @pl.when(fs < high)
                def _():
                    right(kind, j, s).start()

                @pl.when(crosses(kind, j, s))
                def _():
                    across(kind, j, s, rep).start()

            @pl.when((fs + d < nfs) & from_right)
            def _():
                s = fs + d
                left(kind, j, s).wait_recv()

                @pl.when(fs > low)
                def _():
                    left(kind, j, s).start()

                @pl.when(crosses(kind, j, s))
                def _():
                    across(kind, j, s, rep).start()

        loop(first, last, one)

    def complete(kind, j):
        def one(s):
            @pl.when(s != fs)
            def _():
                across(kind, j, s, 1 - rep).wait_recv()

        loop(0, nfs, one)
        local(kind, j).wait()

    def drain(kind, j):
        low, high = ends(kind)

        def one(s):
            @pl.when((s <= fs) & (fs < high))
            def _():
                right(kind, j, s).wait_send()

            @pl.when((s >= fs) & (fs > low))
            def _():
                left(kind, j, s).wait_send()

            inside = (fs >= low) & (fs <= high)

            @pl.when(crosses(kind, j, s) & inside)
            def _():
                across(kind, j, s, rep).wait_send()

        loop(0, nfs, one)

        @pl.when(end & both(kind, j))
        def _():
            extra(kind, j, region(kind, j, fs, 1 - rep)).wait_send()

    def group(to, src, dst, send, recv):
        return pltpu.make_async_remote_copy(
            src, dst, send, recv, device_id={"tp": to}, device_id_type=MESH)

    def up_y(t):
        return lax.rem(y + t, ny) * 2 + core

    def down_y(t):
        return lax.rem(y + ny - t, ny) * 2 + core

    def gathered(j, i, who):
        return big.at[min(j, 1), at(i, LEN), at(who, own)]

    def ag_y(j, i, t):
        src = tokens.at[at(i, LEN), :] if j == 2 else gathered(j, i, tp)
        return group(up_y(t), src, gathered(j, i, tp), ag_send.at[j], ag_recv.at[j, i, tp])

    def ag_pair(j, i):
        src = tokens.at[at(i, LEN), :] if j == 2 else gathered(j, i, tp)
        return group(sibling, src, gathered(j, i, tp), ag_send.at[j], ag_recv.at[j, i, tp])

    def ag_relay(j, i, t):
        who = down_y(t)
        return group(sibling, gathered(j, i, who), gathered(j, i, who), ag_send.at[j], ag_recv.at[j, i, who])

    def ag_start(j, i):
        for t in range(1, ny):
            ag_y(j, i, t).start()
        ag_pair(j, i).start()

    def ag_pass(j, i):
        for t in range(1, ny):
            ag_relay(j, i, t).wait_recv()
            ag_relay(j, i, t).start()

    def ag_finish(j, i):
        for t in range(ny):
            who = lax.rem(y + t, ny) * 2 + 1 - core
            group(sibling, gathered(j, i, who), gathered(j, i, who), ag_send.at[j], ag_recv.at[j, i, who]).wait_recv()

    def ag_drain(j):
        sent = big.at[min(j, 1), :, 0:(2 * ny - 1) * own]
        group(sibling, sent, sent, ag_send.at[j], ag_recv.at[j, 0, tp]).wait_send()

    def hand(i):
        return pltpu.make_async_remote_copy(
            land.at[at(i, LEN), :], land.at[at(i, LEN), :], land_send.at[i], land_recv.at[i],
            device_id={"fs": partner}, device_id_type=MESH)

    def pair_copy(i, b):
        src = active.at[1, at(i, LEN), at(2 * b + 1 - core, own)]
        return group(sibling, src, pair.at[b, at(i, LEN), :], pair_send, pair_recv.at[i, b])

    def rs_copy(i, t):
        src = pair.at[lax.rem(y + t, ny), at(i, LEN), :]
        return group(up_y(t), src, rs.at[t - 1, at(i, LEN), :], rs_send, rs_recv.at[i, t - 1])

    def en_copy(stage, i, t):
        return group(
            lax.rem(tp + t, ntp), energy.at[stage, 0, i], energy.at[stage, t, i],
            en_send, en_recv.at[stage, i])

    def en_put(stage, i, values):
        square = jnp.sum(values * values, axis=1, keepdims=True)
        flat = jnp.transpose(jnp.broadcast_to(square, (LEN, LANES)))
        energy[stage, 0, i] = flat[0:8, :]
        for t in range(1, ntp):
            en_copy(stage, i, t).start()

    def en_get(stage, i):
        others = energy.at[stage, 1:ntp, i]
        group(sibling, others, others, en_send, en_recv.at[stage, i]).wait_recv()
        flat = energy[stage, 0, i]
        for t in range(1, ntp):
            flat = flat + energy[stage, t, i]
        tall = jnp.transpose(jnp.concatenate([flat] * (LANES // 8), axis=0))
        return lax.rsqrt(tall[:, 0:1] / width + epsilon)

    def fp_copy(c, j, i):
        return group(
            sibling, fpart.at[c, j, :, 1 - core, at(i, LEN), :], fpair.at[j, c, :, at(i, LEN), :],
            fp_send, fp_recv.at[j, c, i])

    def fr_copy(c, i, t):
        src = fpair.at[0, c, lax.rem(y + t, ny), at(i, LEN), :]
        return group(up_y(t), src, frs.at[t - 1, c, at(i, LEN), :], fr_send, fr_recv.at[c, i, t - 1])

    def back(c, i):
        return pltpu.make_async_remote_copy(
            fpair.at[1, c, :, at(i, LEN), :], fpair.at[0, c, :, at(i, LEN), :], back_send.at[0], back_recv.at[c, i],
            device_id={"fs": partner}, device_id_type=MESH)

    def send_at(k):
        @pl.when(k == 2)
        def _():
            send_own("mix", 2)

        @pl.when(k == 3)
        def _():
            send_own("out", 0)

        @pl.when((k >= 4) & (k < 4 + nu))
        def _():
            send_own("up", k - 4)

        @pl.when((k >= 4 + nu) & (k < 4 + nu + nc))
        def _():
            send_own("down", k - 4 - nu)

    def relay_at(k, first, last, mid, out):
        @pl.when(k < 3)
        def _():
            relay("mix", k, first, last, mid, out)

        @pl.when(k == 3)
        def _():
            relay("out", 0, first, last, mid, out)

        @pl.when((k >= 4) & (k < 4 + nu))
        def _():
            relay("up", k - 4, first, last, mid, out)

        @pl.when((k >= 4 + nu) & (k < nk))
        def _():
            relay("down", k - 4 - nu, first, last, mid, out)

    def take(q):
        @pl.when(lax.rem(q, 2) == 1)
        def _():
            relay_at((q + 1) // 2, 1, 2, True, False)

        @pl.when(lax.rem(q, 2) == 0)
        def _():
            @pl.when(q // 2 < late)
            def _():
                relay_at(q // 2, 1, 2, q == 0, True)

            send_at(q // 2 + 2 + jnp.where(q >= 8, 1, 0))

            @pl.when(q == 6)
            def _():
                send_at(6)

            @pl.when((q >= 2) & (q // 2 - 1 < late))
            def _():
                relay_at(q // 2 - 1, 2, nfs, True, True)

    def takes(low, high):
        @pl.when(worker)
        def _():
            with jax.named_scope("take"):
                loop(low, high, take)

    def outer_mix(*parts):
        @pl.when(jnp.logical_not(worker))
        def _():
            for d, k in parts:
                kind, j = ("mix", k) if k < 3 else ("out", 0)
                with jax.named_scope("relay"):
                    relay(kind, j, d, d + 1 if d < 3 else nfs)

    def send_outer(low, high):
        @pl.when(jnp.logical_not(worker))
        def _():
            loop(4 + low, 4 + min(high, nu + nc), send_at)

    def fs_copy(c, i, t):
        src = fpair.at[1, c, lax.rem(y + t, ny), at(i, LEN), :]
        dst = fsum.at[t - 1, c - n_direct, at(i, LEN), :]
        return group(up_y(t), src, dst, fs_send, fs_recv.at[c, i, t - 1])

    def back_own(c, i):
        return pltpu.make_async_remote_copy(
            fpair.at[1, c, y, at(i, LEN), :], fpair.at[0, c, y, at(i, LEN), :], back_send.at[1], back_recv.at[c, i],
            device_id={"fs": partner}, device_id_type=MESH)

    send_own("mix", 0)
    loop(0, seqs, lambda i: ag_start(2, i))
    own_tok = pltpu.make_async_copy(tokens, big.at[1, :, at(tp, own)], tok_local)
    own_tok.start()
    send_own("mix", 1)

    @pl.when(jnp.logical_not(worker))
    def _():
        send_own("mix", 2)
        send_own("out", 0)

    for k in range(3):
        local("mix", k).start()
    local("out", 0).start()

    @pl.when(worker)
    def _():
        loop(0, nu, lambda j: local("up", j).start())
        loop(0, nc, lambda j: local("down", j).start())

    takes(0, 3)
    outer_mix((1, 0), (1, 1), (2, 0), (1, 2))
    takes(3, 4)
    with jax.named_scope("tok_pass"):
        loop(0, seqs, lambda i: ag_pass(2, i))
    takes(4, 5)
    outer_mix((2, 1), (3, 0), (1, 3))
    send_outer(0, 2)
    own_tok.wait()

    def norm_tokens(i):
        ag_finish(2, i)
        r = at(i, LEN)
        v = big[1, r, :].astype(F32)
        factor = lax.rsqrt(jnp.mean(v * v, axis=-1, keepdims=True) + epsilon)
        big[0, r, :] = (v * factor * row(gain1[...])).astype(BF16)

    with jax.named_scope("norm"):
        loop(0, seqs, norm_tokens)
    takes(5, 7)
    outer_mix((2, 2), (3, 1), (2, 3))
    send_outer(2, nu)
    outer_mix((3, 2), (3, 3))
    send_outer(nu, nu + min(2, nc))
    with jax.named_scope("mix_wait"):
        for k in range(3):
            complete("mix", k)

    own_taps = taps[:, at(tp, chan)].astype(F32)
    position = lax.broadcasted_iota(jnp.int32, (LEN, chan), 0)

    def mixer(i):
        r = at(i, LEN)
        rows = big[0, r, :]
        inner = dot(rows, rows_w[1]).astype(BF16).astype(F32) * dot(rows, rows_w[2]).astype(BF16).astype(F32)
        before = jnp.where(position == 0, 0.0, pltpu.roll(inner, 1, 0))
        after = jnp.where(position == LEN - 1, 0.0, pltpu.roll(inner, LEN - 1, 0))
        conv = own_taps[0:1] * before + own_taps[1:2] * inner + own_taps[2:3] * after
        outer = dot(rows, rows_w[0]).astype(BF16).astype(F32)
        active[0, r, 0:chan] = (outer * conv).astype(BF16)

    def project(i):
        r = at(i, LEN)
        active[1, r, 0:width] = dot(active[0, r, 0:chan], out_w[...]).astype(BF16)
        for b in range(ny):
            pair_copy(i, b).start()

    def chip_sum(i):
        r = at(i, LEN)
        for b in range(ny):
            pair_copy(i, b).wait_recv()
            total = active[1, r, at(2 * b + core, own)].astype(F32) + pair[b, r, :].astype(F32)
            pair[b, r, :] = total.astype(BF16)

    def rs_start(i):
        for t in range(1, ny):
            rs_copy(i, t).start()

    def mix(step):
        @pl.when(step < seqs)
        def _():
            with jax.named_scope("mixer"):
                mixer(step)

        @pl.when(step == 1)
        def _():
            takes(8, 9)

        @pl.when(step == 2)
        def _():
            takes(7, 8)
            takes(9, 10)
            with jax.named_scope("out_wait"):
                complete("out", 0)

        @pl.when((step >= 2) & (step < seqs + 2))
        def _():
            with jax.named_scope("project"):
                project(step - 2)

        @pl.when(step >= 3)
        def _():
            with jax.named_scope("chip_sum"):
                chip_sum(step - 3)

        @pl.when((step == 3) | (step == 4))
        def _():
            rs_start(step - 3)

    loop(0, seqs + 3, mix)
    takes(10, 11)
    ag_drain(2)
    group(sibling, active.at[1, :, 0:ny * own], active.at[1, :, 0:ny * own], pair_send, pair_recv.at[0, 0]).wait_send()

    own_gain2 = row(gain2[at(tp, own)])
    own_gain3 = row(gain3[at(tp, own)])

    def mixed_sum(i):
        r = at(i, LEN)
        total = pair[y, r, :].astype(F32)
        for t in range(1, ny):
            rs_copy(i, t).wait_recv()
            total = total + rs[t - 1, r, :].astype(F32)
        acc[r, :] = total
        en_put(0, i, total)

    def add_resid(i):
        r = at(i, LEN)
        scale = en_get(0, i)
        res = (big[1, r, at(tp, own)].astype(F32) + acc[r, :] * scale * own_gain2).astype(BF16)
        resid[r, :] = res
        en_put(1, i, res.astype(F32))

    def normalise(i):
        r = at(i, LEN)
        rows = (resid[r, :].astype(F32) * en_get(1, i) * own_gain3).astype(BF16)

        @pl.when(worker)
        def _():
            big[0, r, at(tp, own)] = rows
            ag_start(0, i)

        @pl.when(jnp.logical_not(worker))
        def _():
            land[r, :] = rows
            hand(i).start()

    def lift(j, i):
        ag_finish(j, i)
        r = at(i, LEN)
        rows = big[j, r, :]
        for u in range(nu):
            lifted = jnp.maximum(dot(rows, rows_w[3 + u]), 0.0)
            active[j, r, pl.ds(u * ucol, ucol)] = (lifted * lifted).astype(BF16)

    def exchange(step):
        takes(11 + step, 12 + step)

        @pl.when(step < seqs)
        def _():
            with jax.named_scope("mixed_sum"):
                mixed_sum(step)

        @pl.when((step >= 1) & (step < seqs + 1))
        def _():
            with jax.named_scope("add_resid"):
                add_resid(step - 1)

        @pl.when((step >= 2) & (step < seqs + 2))
        def _():
            with jax.named_scope("normalise"):
                normalise(step - 2)

        @pl.when(step + 2 < seqs)
        def _():
            rs_start(step + 2)

        @pl.when(step < 3)
        def _():
            drain("mix", step)

    def spread(step):
        @pl.when(step < 3)
        def _():
            takes(taken + step, taken + step + 1)

        @pl.when(step < seqs)
        def _():
            with jax.named_scope("ag_pass0"):
                ag_pass(0, step)

        @pl.when(step == 1)
        def _():
            with jax.named_scope("up_wait"):
                loop(0, nu, lambda j: complete("up", j))

        @pl.when(step >= 1)
        def _():
            with jax.named_scope("lift0"):
                lift(0, step - 1)

    loop(0, max(seqs + 2, 3), exchange)
    taken = 11 + max(seqs + 2, 3)
    send_outer(nu + min(2, nc), nu + nc)
    drain("out", 0)

    @pl.when(worker)
    def _():
        loop(0, seqs + 1, spread)

    taken += min(seqs + 1, 3)

    def sum_pair(c, j, i):
        r = at(i, LEN)
        fp_copy(c, j, i).wait_recv()
        for b in range(ny):
            total = fpart[c, j, b, core, r, :].astype(F32) + fpair[j, c, b, r, :].astype(F32)
            fpair[j, c, b, r, :] = total.astype(BF16)

    def fr_start(c, i):
        for t in range(1, ny):
            fr_copy(c, i, t).start()

    @pl.when(jnp.logical_not(worker))
    def _():
        loop(0, nu, lambda j: drain("up", j))

        frs[:, n_direct:] = jnp.zeros((ny - 1, nc - n_direct, count, piece), BF16)

        def returned(c):
            def one(i):
                back(c, i).wait_recv()
                fr_start(c, i)

            loop(0, seqs, one)

        with jax.named_scope("returned"):
            loop(0, n_direct, returned)

    @pl.when(worker)
    def _():
        lag = 2
        total = 2 * nk + 1

        def unit(c, j, i):
            r = at(i, LEN)
            product = dot(active[j, r, 0:hidden], down_w[c]).astype(BF16)
            for b in range(ny):
                for odd_ in range(2):
                    lane = (2 * b + odd_) * piece
                    fpart[c, j, b, odd_, r, :] = product[:, lane:lane + piece]
            fp_copy(c, j, i).start()

        def post(c, j, i, go=True):
            sum_pair(c, j, i)

            @pl.when((j == 0) & go)
            def _():
                fr_start(c, i)

            @pl.when((j == 1) & (c < n_direct))
            def _():
                back(c, i).start()

            @pl.when((j == 1) & (c >= n_direct))
            def _():
                for t in range(1, ny):
                    fs_copy(c, i, t).start()

        def units(c, j, go=True):
            def one(n):
                @pl.when(n < seqs)
                def _():
                    unit(c, j, n)

                @pl.when(n >= lag)
                def _():
                    post(c, j, n - lag, go)

            with jax.named_scope("units"):
                loop(0, seqs + lag, one)

        def chunk(c):
            with jax.named_scope("down_wait"):
                complete("down", c)

        def late_near(k):
            with jax.named_scope("late"):
                relay_at(k, 1, 2, False, True)

        def late_far(k):
            with jax.named_scope("late"):
                relay_at(k, 2, nfs, True, True)

        def client(step):
            @pl.when(step < seqs)
            def _():
                with jax.named_scope("hand_wait"):
                    hand(step).wait_recv()
                r = at(step, LEN)
                big[1, r, at(tp, own)] = land[r, :]
                ag_start(1, step)

            @pl.when((step == 0) & (n_early > 0))
            def _():
                chunk(0)
                units(0, 0, False)

            @pl.when((step >= 1) & (step < seqs + 1))
            def _():
                with jax.named_scope("ag_pass1"):
                    ag_pass(1, step - 1)

            takes(jnp.minimum(reached + step, total), jnp.minimum(reached + step + 1, total))

            @pl.when((step >= 3) & (late + step - 3 < nk))
            def _():
                late_near(late + step - 3)

            @pl.when((step >= 5) & (late + step - 5 < nk))
            def _():
                late_far(late + step - 5)

            @pl.when(step >= 2)
            def _():
                i = step - 2
                with jax.named_scope("lift1"):
                    lift(1, i)

                @pl.when(step == 2)
                def _():
                    for c in range(1, n_early):
                        chunk(c)

                @pl.when(step == seqs)
                def _():
                    if n_early > 0:
                        loop(0, seqs, lambda i: fr_start(0, i))

                with jax.named_scope("early"):
                    loop(0, n_early, lambda c: unit(c, 1, i))
                    loop(0, n_early, lambda c: post(c, 1, i))

        reached = max(taken, 2 * (4 + nu) + 2 + n_early) if nc > 1 else taken
        takes(taken, reached)
        loop(0, seqs + 2, client)
        takes(min(reached + seqs + 2, total), total)
        loop(min(late + seqs - 1, nk), nk, late_near)
        loop(min(late + seqs - 3, nk), nk, late_far)

        def gather(c, i):
            r = at(i, LEN)
            sums = fpair[1, c, y, r, :].astype(F32)
            for t in range(1, ny):
                fs_copy(c, i, t).wait_recv()
                sums = sums + fsum[t - 1, c - n_direct, r, :].astype(F32)
            fpair[1, c, y, r, :] = sums.astype(BF16)
            back_own(c, i).start()

        own_left = list(range(1, nc)) if n_early else list(range(nc))
        while own_left and own_left[0] < n_early:
            units(own_left.pop(0), 0)
        for c in range(n_early, nc):
            chunk(c)
            units(c, 1)
        while own_left:
            if len(own_left) == 1:
                with jax.named_scope("gather"):
                    loop(n_direct, nc, lambda c: loop(0, seqs, lambda i: gather(c, i)))
            units(own_left.pop(0), 0)
        loop(0, nu, lambda j: drain("up", j))

    own_gain4 = row(gain4[at(tp, own)])

    def close(step):
        @pl.when(step < seqs)
        def _():
            r = at(step, LEN)
            parts = []
            for c in range(nc):
                if c >= n_direct:
                    @pl.when(jnp.logical_not(worker))
                    def _():
                        back_own(c, step).wait_recv()
                total = fpair[0, c, y, r, :].astype(F32)
                for t in range(1, ny):
                    @pl.when(worker | (c < n_direct))
                    def _():
                        fr_copy(c, step, t).wait_recv()
                    total = total + frs[t - 1, c, r, :].astype(F32)
                parts.append(total)
            total = parts[0] if nc == 1 else jnp.concatenate(parts, axis=1)
            acc[r, :] = total
            en_put(2, step, total)

        @pl.when(step > 0)
        def _():
            r = at(step - 1, LEN)
            scale = en_get(2, step - 1)
            result[r, :] = (resid[r, :].astype(F32) + acc[r, :] * scale * own_gain4).astype(BF16)

    with jax.named_scope("close"):
        loop(0, seqs + 1, close)

    with jax.named_scope("drain"):
        loop(0, nc, lambda j: drain("down", j))

    def sent(ref, sem):
        group(sibling, ref, ref, sem, pair_recv.at[0, 0]).wait_send()

    with jax.named_scope("finish"):
        sent(rs, rs_send)
        sent(energy.at[:, 1:ntp], en_send)

        @pl.when(worker)
        def _():
            ag_drain(0)
            ag_drain(1)
            sent(fpair, fp_send)
            sent(frs, fr_send)
            sent(fsum, fs_send)
            sent(fpair.at[1, n_direct:nc, 0], back_send.at[1])
            if n_direct > 0:
                sent(fpair.at[1, 0:n_direct], back_send.at[0])

        @pl.when(jnp.logical_not(worker))
        def _():
            if n_direct > 0:
                sent(frs.at[:, 0:n_direct], fr_send)
            loop(0, seqs, lambda i: hand(i).wait_send())


def solution(mesh):
    nfs, ntp = mesh.shape["fs"], mesh.shape["tp"]
    assert mesh.shape["rep"] == 2 and nfs % 2 == 0 and nfs >= 4 and ntp % 2 == 0

    def body(tokens, gain1, wb, wc, wv, taps, wo, gain2, gain3, wu, wd, gain4):
        count, own = tokens.shape
        width, chan, hidden = own * ntp, wb.shape[1], wu.shape[1]
        nu = hidden // chan
        cw = min(LANES, wd.shape[1])
        nc = wd.shape[1] // cw
        nk = 4 + nu + nc
        ny, seqs = ntp // 2, count // LEN
        piece = nfs * cw // ntp
        vm, anyw = pl.BlockSpec(memory_space=pltpu.VMEM), pl.BlockSpec(memory_space=pl.ANY)
        dma = pltpu.SemaphoreType.DMA
        return pl.pallas_call(
            functools.partial(kernel, nfs, ntp, nu, nc, cw),
            out_shape=jax.ShapeDtypeStruct((count, own), BF16),
            in_specs=[anyw, vm, anyw, anyw, anyw, vm, anyw, vm, vm, anyw, anyw, vm],
            out_specs=vm,
            scratch_shapes=[
                pltpu.VMEM((3 + nu, width, chan), BF16),
                pltpu.VMEM((chan, width), BF16),
                pltpu.VMEM((nc, hidden, nfs * cw), BF16),
                pltpu.VMEM((2, count, width), BF16),
                pltpu.VMEM((2, count, max(hidden, width)), BF16),
                pltpu.VMEM((count, own), BF16),
                pltpu.VMEM((ny, count, own), BF16),
                pltpu.VMEM((ny - 1, count, own), BF16),
                pltpu.VMEM((count, own), F32),
                pltpu.VMEM((count, own), BF16),
                pltpu.VMEM((nc, 2, ny, 2, count, piece), BF16),
                pltpu.VMEM((2, nc, ny, count, piece), BF16),
                pltpu.VMEM((ny - 1, nc, count, piece), BF16),
                pltpu.VMEM((ny - 1, nc - direct_chunks(nc), count, piece), BF16),
                pltpu.VMEM((3, ntp, seqs, 8, LEN), F32),
                dma((nk, nfs)), dma((nk, nfs)), dma((nk, nfs)), dma((nk, nfs)), dma((nk, nfs)),
                dma((nk,)), dma,
                dma((3,)), dma((3, seqs, ntp)), dma((seqs,)), dma((seqs,)),
                dma, dma((seqs, ny)), dma, dma((seqs, ny - 1)),
                dma, dma((3, seqs)),
                dma, dma((2, nc, seqs)), dma, dma((nc, seqs, ny - 1)),
                dma((2,)), dma((nc, seqs)), dma, dma((nc, seqs, ny - 1)),
            ],
            compiler_params=pltpu.CompilerParams(
                collective_id=0, has_side_effects=True, vmem_limit_bytes=67043328),
            name="layer",
        )(tokens, gain1, wb, wc, wv, taps, wo, gain2, gain3, wu, wd, gain4)

    placed = (
        P(("rep", "fs"), "tp"), P(), P("fs", "tp"), P("fs", "tp"), P("fs", "tp"), P(), P("tp", "fs"),
        P(), P(), P("fs", "tp"), P("tp", "fs"), P(),
    )
    return jax.shard_map(
        body, mesh=mesh, in_specs=placed, out_specs=P(("rep", "fs"), "tp"), check_vma=False
    )
```
